32 devices in a mesh: sp: 8 (over z, y), tp: 4 (over x, core).
Axes of the slice: x: 2, y: 2, z: 4, core: 2. Of those that a mesh axis runs over, the one named last changes fastest.
Arguments:
- residual_input_stream: bfloat16 [6144, 2048], P('sp'), may hold values from -6 to 6
- projected_queries: bfloat16 [6144, 512], P('sp', 'tp'), may hold values from -6 to 6
- projected_keys: bfloat16 [6144, 512], P('sp', 'tp'), may hold values from -6 to 6
- projected_values: bfloat16 [6144, 1024], P('sp', 'tp'), may hold values from -6 to 6
- emitted_switch_entries: bfloat16 [6144, 1024], P('sp', 'tp'), may hold values from -6 to 6
- retention_preactivations: bfloat16 [6144, 512], P('sp', 'tp'), may hold values from -6 to 15
- additional_fading_amount: float32 [6144], P('sp'), may hold values from -2 to 0
- head_norm_gain: float32 [128], replicated, may hold values from 0.1 to 1.9
- attention_output_weight: bfloat16 [1024, 2048], P('tp'), may hold values from -0.1875 to 0.1875
- feedforward_norm_gain: float32 [2048], replicated, may hold values from 0.1 to 1.9
- gate_up_matrix: bfloat16 [2048, 5632], P('sp', 'tp'), may hold values from -0.125 to 0.125
- value_up_matrix: bfloat16 [2048, 5632], P('sp', 'tp'), may hold values from -0.125 to 0.125
- gate_filter_taps: bfloat16 [3, 5632], P(None, 'tp'), may hold values from -3.5 to 3.5
- value_filter_taps: bfloat16 [3, 5632], P(None, 'tp'), may hold values from -3.5 to 3.5
- down_projection_weight: bfloat16 [5632, 2048], P('tp', 'sp'), may hold values from -0.078125 to 0.078125
Outputs:
- layer_out: bfloat16 [6144, 2048], P(('sp', 'tp'))
The draws below stay inside these ranges and needn't reach their ends.
All inputs are finite; a program needn't handle non-finite values.
Results may differ from the reference program's by a relative error of at most 0.011.
Values may be sent and summed in bfloat16 or wider, within the bound.
A program may use at most 128 MiB of HBM per device.

```python
import math
import jax
import jax.numpy as jnp
from jax import lax

D = 2048
HEADS = 8
DK = 64
DV = 128
FF = 5632
CONV = 3
BLOCK = 64
TOK_DEV = 768
KW = 512
VW = 1024
TOKENS = 6144


def draw_retention_preactivations(key, part):
    keys_all = jax.random.split(jax.random.fold_in(key, 11), 3)
    ranking = jax.random.permutation(keys_all[0], HEADS)
    fast_count = HEADS // 2
    channel_head = jnp.arange(HEADS * DK) // DK
    head_fast = (ranking < fast_count).astype(jnp.float32)
    chan_fast = jnp.sum((channel_head[:, None] == jnp.arange(HEADS)[None, :]).astype(jnp.float32) * head_fast[None, :], axis=1)
    slow_base = math.log(TOKENS) - 1.6
    base = chan_fast + (1.0 - chan_fast) * slow_base
    device_count = TOKENS // TOK_DEV
    shifts = jax.random.uniform(keys_all[1], (device_count,), jnp.float32, -1.0, 1.0)
    position_dev = jnp.arange(TOKENS) // TOK_DEV
    shift_rows = jnp.sum((position_dev[:, None] == jnp.arange(device_count)[None, :]).astype(jnp.float32) * shifts[None, :], axis=1)
    noise = jnp.clip(jax.random.normal(keys_all[2], (TOKENS, HEADS * DK), jnp.float32), -5.0, 5.0)
    return (base[None, :] + shift_rows[:, None] + noise).astype(jnp.bfloat16)


def draw_additional_fading_amount(key, part):
    keys_all = jax.random.split(jax.random.fold_in(key, 23), 2)
    places = jax.random.randint(keys_all[0], (3,), 0, TOKENS)
    depths = jnp.log(jax.random.uniform(keys_all[1], (3,), jnp.float32, 0.5, 0.8))
    marks = (jnp.arange(TOKENS)[:, None] == places[None, :]).astype(jnp.float32)
    return jnp.sum(marks * depths[None, :], axis=1).astype(jnp.float32)


def levels(key, extent, shards, low, top_value):
    level = 1.0
    for position, parts in shards:
        steps = jax.random.uniform(jax.random.fold_in(jax.random.fold_in(key, 6), position), (parts,), jnp.float32, low / len(shards), top_value / len(shards))
        level = level * jnp.repeat(jnp.exp(steps), extent[position] // parts).reshape((-1,) + (1,) * (len(extent) - 1 - position))
    return level


def normal_values(stream_key, shape, scale, reach, pieces=(), kind=jnp.bfloat16):
    entries = jax.random.normal(stream_key, shape, jnp.float32) * scale
    if len(pieces) > 0:
        entries = levels(stream_key, shape, pieces, -0.22, 0.18) * entries
    return jnp.clip(entries, min=-reach, max=reach).astype(kind)


def setup_inputs(seed: int = 0) -> dict:
    seeds = jax.random.split(jax.random.key(seed), 16)
    residual_input_stream = normal_values(seeds[0], (TOKENS, D), 1.0, 6.0, ((0, 8),))
    projected_queries = normal_values(seeds[1], (TOKENS, KW), 1.0, 6.0, ((0, 8), (1, 4)))
    projected_keys = normal_values(seeds[2], (TOKENS, KW), 1.0, 6.0, ((0, 8), (1, 4)))
    projected_values = normal_values(seeds[3], (TOKENS, VW), 1.0, 6.0, ((0, 8), (1, 4)))
    emitted_switch_entries = normal_values(seeds[4], (TOKENS, VW), 1.0, 6.0, ((0, 8), (1, 4)))
    retention_preactivations = draw_retention_preactivations(jax.random.fold_in(seeds[15], 71), 0)
    additional_fading_amount = draw_additional_fading_amount(jax.random.fold_in(seeds[15], 71), 0)
    head_norm_gain = jnp.clip(1.0 + 0.18 * jax.random.normal(seeds[7], (DV,), jnp.float32), 0.1, 1.9)
    attention_output_weight = normal_values(seeds[8], (VW, D), VW ** -0.5, 0.1875, ((0, 4),))
    feedforward_norm_gain = jnp.clip(1.0 + 0.18 * jax.random.normal(seeds[9], (D,), jnp.float32), 0.1, 1.9)
    gate_up_matrix = normal_values(seeds[10], (D, FF), D ** -0.5, 0.125, ((0, 8), (1, 4)))
    value_up_matrix = normal_values(seeds[11], (D, FF), D ** -0.5, 0.125, ((0, 8), (1, 4)))
    gate_filter_taps = normal_values(seeds[12], (CONV, FF), CONV ** -0.5, 3.5, ((1, 4),))
    value_filter_taps = normal_values(seeds[13], (CONV, FF), CONV ** -0.5, 3.5, ((1, 4),))
    down_projection_weight = normal_values(seeds[14], (FF, D), FF ** -0.5, 0.078125, ((0, 4), (1, 8)))
    return dict(residual_input_stream=residual_input_stream, projected_queries=projected_queries, projected_keys=projected_keys, projected_values=projected_values, emitted_switch_entries=emitted_switch_entries, retention_preactivations=retention_preactivations, additional_fading_amount=additional_fading_amount, head_norm_gain=head_norm_gain, attention_output_weight=attention_output_weight, feedforward_norm_gain=feedforward_norm_gain, gate_up_matrix=gate_up_matrix, value_up_matrix=value_up_matrix, gate_filter_taps=gate_filter_taps, value_filter_taps=value_filter_taps, down_projection_weight=down_projection_weight)


eps = 1e-06
retention_sharpness = 16.0

def to_blocks(tensor, width):
    count = tensor.shape[0] // BLOCK
    return tensor.astype(jnp.float32).reshape(count, BLOCK, HEADS, width)

def depthwise(upward, taps):
    length = upward.shape[0]
    padded = jnp.concatenate([jnp.zeros((CONV - 1, upward.shape[1]), jnp.bfloat16), upward], axis=0)
    result = jnp.zeros(upward.shape, jnp.float32)
    for offset in range(CONV):
        result = result + taps[offset].astype(jnp.float32)[None] * padded[offset:offset + length].astype(jnp.float32)
    return result

def reference(residual_input_stream, projected_queries, projected_keys, projected_values, emitted_switch_entries, retention_preactivations, additional_fading_amount, head_norm_gain, attention_output_weight, feedforward_norm_gain, gate_up_matrix, value_up_matrix, gate_filter_taps, value_filter_taps, down_projection_weight):
    largest_exponent = lax.Precision.HIGHEST
    retention_logarithm = jax.nn.log_sigmoid(retention_preactivations.astype(jnp.float32)) / retention_sharpness + additional_fading_amount[:, None]
    scaled_q = to_blocks(projected_queries, DK) * DK ** (-0.5)
    key_heads = to_blocks(projected_keys, DK)
    value_heads = to_blocks(projected_values, DV)
    rate_cum = jnp.cumsum(to_blocks(retention_logarithm, DK), axis=1)
    block_total = rate_cum[:, -1]
    q_decayed = scaled_q * jnp.exp(rate_cum)
    k_growth = key_heads * jnp.exp(-rate_cum)
    fading_through_finish = key_heads * jnp.exp(block_total[:, None] - rate_cum)
    lower = jnp.tril(jnp.ones((BLOCK, BLOCK), bool))
    scores = jnp.einsum('nihk,njhk->nhij', q_decayed, k_growth, precision=largest_exponent)
    scores = jnp.where(lower[None, None], scores, 0.0)
    within = jnp.einsum('nhij,njhv->nihv', scores, value_heads, precision=largest_exponent)
    increments = jnp.einsum('nchk,nchv->nhkv', fading_through_finish, value_heads, precision=largest_exponent)

    def advance_recurrence(state, inputs):
        factor, increment = inputs
        return (factor[..., None] * state + increment, state)
    start_state = jnp.zeros((HEADS, DK, DV), jnp.float32)
    final_state, state_before = lax.scan(advance_recurrence, start_state, (jnp.exp(block_total), increments))
    earlier = jnp.einsum('nchk,nhkv->nchv', q_decayed, state_before, precision=largest_exponent)
    mech_out = (within + earlier).reshape(TOKENS, HEADS, DV)
    mech_out = mech_out * lax.rsqrt(lax.optimization_barrier(jnp.mean(mech_out * mech_out, axis=-1, keepdims=True)) + eps) * head_norm_gain
    mixed = (mech_out.reshape(TOKENS, VW) * jax.nn.silu(emitted_switch_entries.astype(jnp.float32))).astype(jnp.bfloat16)
    attended = jnp.dot(mixed, attention_output_weight, preferred_element_type=jnp.float32)
    resid = residual_input_stream.astype(jnp.float32) + attended
    normed = (resid * lax.rsqrt(lax.optimization_barrier(jnp.mean(resid * resid, axis=-1, keepdims=True)) + eps) * feedforward_norm_gain).astype(jnp.bfloat16)
    gate_up = jnp.dot(normed, gate_up_matrix, preferred_element_type=jnp.float32).astype(jnp.bfloat16)
    value_up = jnp.dot(normed, value_up_matrix, preferred_element_type=jnp.float32).astype(jnp.bfloat16)
    gate_mix = depthwise(gate_up, gate_filter_taps)
    value_mix = depthwise(value_up, value_filter_taps)
    hidden = (jax.nn.silu(gate_mix) * value_mix).astype(jnp.bfloat16)
    return (resid + jnp.dot(hidden, down_projection_weight, preferred_element_type=jnp.float32)).astype(jnp.bfloat16)
```

```python
import jax
import jax.numpy as jnp
from jax import lax
from jax.sharding import Mesh, PartitionSpec as P

DK = 64
DV = 128
CONV = 3
BLOCK = 64
EDGE = 16
SP = ("so", "si")


eps = 1e-06
retention_sharpness = 16.0


def from_behind(block, axis, distance):
    devices = range(lax.axis_size(axis))
    route = [(i - distance, i) for i in devices if i - distance in devices]
    return lax.ppermute(block, axis, route)


def to_blocks(tensor, local_heads, width):
    count = tensor.shape[0] // BLOCK
    return tensor.astype(jnp.float32).reshape(count, BLOCK, local_heads, width)


def row_norm(stream, gain):
    scaled = stream * lax.rsqrt(jnp.mean(stream * stream, axis=-1, keepdims=True) + eps)
    return (scaled * gain).astype(jnp.bfloat16)


def state_before_device(dev_log, dev_state):
    heads, channels, width = dev_state.shape
    lanes = heads * channels
    decay = jnp.pad(jnp.exp(dev_log).reshape(1, lanes), ((0, 0), (0, -lanes % width)))
    decay = decay.reshape(-1, width)
    packed = jnp.concatenate([dev_state.reshape(lanes, width), decay], axis=0)
    arriving = jnp.zeros_like(dev_state)
    after = jnp.ones((heads, channels), jnp.float32)
    for distance in range(1, lax.axis_size("so") * lax.axis_size("si")):
        got = from_behind(packed, SP, distance)
        arriving = arriving + after[..., None] * got[:lanes].reshape(dev_state.shape)
        after = after * got[lanes:].reshape(-1)[:lanes].reshape(after.shape)
    return arriving


def xor_route(axis, bit):
    return [(i, i ^ bit) for i in range(lax.axis_size(axis))]


def exchange(block, axis, bit):
    return lax.ppermute(block, axis, xor_route(axis, bit))


def gather_tp(block):
    count, me = lax.axis_size("tp"), lax.axis_index("tp")
    held = block[None]
    bit = count // 2
    while bit:
        other = exchange(held, "tp", bit)
        low = (me & bit) == 0
        held = jnp.stack([jnp.where(low, held, other), jnp.where(low, other, held)])
        held = held.reshape((-1,) + block.shape)
        bit //= 2
    bits = count.bit_length() - 1
    order = [sum(((t >> b) & 1) << (bits - 1 - b) for b in range(bits)) for t in range(count)]
    return [held[o] for o in order]


def swap_halves(block):
    first = lax.axis_index("si") == 0
    half = block.shape[0] // 2
    low, high = block[:half], block[half:]
    keep, give = jnp.where(first, low, high), jnp.where(first, high, low)
    got = exchange(give, "si", 1)
    return jnp.concatenate([jnp.where(first, keep, got), jnp.where(first, got, keep)], axis=1)


def line_gather(block):
    count, me = lax.axis_size("so"), lax.axis_index("so")
    if count != 4:
        whole = lax.all_gather(block, "so", axis=0)
        return [lax.dynamic_index_in_dim(whole, (me + k) % count, 0, False) for k in range(count)]
    across = lax.ppermute(block, "so", [(i, i ^ 2) for i in range(4)])
    above = lax.ppermute(block, "so", [(1, 0), (2, 1), (3, 2)])
    below = lax.ppermute(block, "so", [(0, 1), (1, 2), (2, 3)])
    far = lax.ppermute(across, "so", [(1, 0), (2, 3)])
    return [block, jnp.where(me == 3, far, above), across, jnp.where(me == 0, far, below)]


def pair_rows(normed):
    share = normed.shape[0] // 2
    mine = lax.axis_index("tp") % 2
    part = exchange(lax.dynamic_slice_in_dim(normed, mine * share, share, 0), "si", 1)
    other = exchange(part, "tp", 1)
    first = mine == 0
    return jnp.concatenate([jnp.where(first, part, other), jnp.where(first, other, part)], axis=0)


def project(rows, lines, width):
    count, me = lax.axis_size("so"), lax.axis_index("so")
    total = 0.0
    for k, line in enumerate(lines):
        part = lax.dynamic_slice_in_dim(rows, (me + k) % count * width, width, 1)
        total = total + lax.dot_general(
            part, line, (((1,), (1,)), ((), ())), preferred_element_type=jnp.float32
        )
    return total.astype(jnp.bfloat16)


def depthwise(before, body, taps):
    padded = jnp.concatenate([before, body], axis=0)
    start = padded.shape[0] - body.shape[0] - (CONV - 1)
    result = jnp.zeros(body.shape, jnp.float32)
    for offset in range(CONV):
        result = result + taps[offset].astype(jnp.float32)[None] * padded[
            start + offset : start + offset + body.shape[0]
        ].astype(jnp.float32)
    return result


def my_half(taps):
    half = taps.shape[1] // 2
    return jnp.where(lax.axis_index("si") == 0, taps[:, :half], taps[:, half:])


def halve(held, axis, bit):
    mine = (lax.axis_index(axis) // bit) % 2
    keep = lax.dynamic_index_in_dim(held, mine, 1, False)
    give = lax.dynamic_index_in_dim(held, 1 - mine, 1, False)
    got = exchange(give.astype(jnp.bfloat16), axis, bit)
    return keep.astype(jnp.float32) + got.astype(jnp.float32)


def scatter_sum(own, other):
    count = lax.axis_size("tp")
    share = own.shape[0] // count
    held = jnp.concatenate([own, other], axis=0)
    held = halve(held.reshape(count, 2, share, -1), "tp", 1)
    held = held.reshape(2, count // 2, share, -1)
    got = exchange(held[1].astype(jnp.bfloat16), "si", 1)
    held = held[0] + got.astype(jnp.float32)
    bit = 2
    while bit < count:
        held = halve(held.reshape((-1, 2) + held.shape[1:]), "tp", bit)
        bit *= 2
    return held[0]


def per_device(
    residual_input_stream,
    projected_queries,
    projected_keys,
    projected_values,
    emitted_switch_entries,
    retention_preactivations,
    additional_fading_amount,
    head_norm_gain,
    attention_output_weight,
    feedforward_norm_gain,
    gate_up_matrix,
    value_up_matrix,
    gate_filter_taps,
    value_filter_taps,
    down_projection_weight,
):
    largest_exponent = lax.Precision.HIGHEST
    tok_rows = residual_input_stream.shape[0]
    local_heads = projected_queries.shape[1] // DK
    gate_lines = line_gather(swap_halves(gate_up_matrix.T))
    value_lines = line_gather(swap_halves(value_up_matrix.T))
    down_lines = line_gather(swap_halves(down_projection_weight))
    out_full = jnp.concatenate(gather_tp(attention_output_weight), axis=0)
    retention_logarithm = (
        jax.nn.log_sigmoid(retention_preactivations.astype(jnp.float32)) / retention_sharpness
        + additional_fading_amount[:, None]
    )
    scaled_q = to_blocks(projected_queries, local_heads, DK) * DK ** (-0.5)
    key_heads = to_blocks(projected_keys, local_heads, DK)
    value_heads = to_blocks(projected_values, local_heads, DV)
    rate_cum = jnp.cumsum(to_blocks(retention_logarithm, local_heads, DK), axis=1)
    block_total = rate_cum[:, -1]
    before_block = jnp.cumsum(block_total, axis=0) - block_total
    q_decayed = scaled_q * jnp.exp(rate_cum)
    k_growth = key_heads * jnp.exp(-rate_cum)
    fading_through_finish = key_heads * jnp.exp(block_total[:, None] - rate_cum)
    lower = jnp.tril(jnp.ones((BLOCK, BLOCK), bool))
    scores = jnp.einsum("nihk,njhk->nhij", q_decayed, k_growth, precision=largest_exponent)
    scores = jnp.where(lower[None, None], scores, 0.0)
    within = jnp.einsum("nhij,njhv->nihv", scores, value_heads, precision=largest_exponent)
    increments = jnp.einsum(
        "nchk,nchv->nhkv", fading_through_finish, value_heads, precision=largest_exponent
    )

    count = block_total.shape[0]
    ends = before_block + block_total
    reached = jnp.concatenate([before_block, ends[-1:]], axis=0)
    earlier_block = jnp.arange(count)[None, :] < jnp.arange(count + 1)[:, None]
    fade = jnp.where(
        earlier_block[..., None, None],
        jnp.exp(jnp.minimum(reached[:, None] - ends[None], 0.0)),
        0.0,
    )
    states = jnp.sum(fade[..., None] * increments[None], axis=1)
    state_before, dev_state = states[:-1], states[-1]
    earlier = jnp.einsum("nchk,nhkv->nchv", q_decayed, state_before, precision=largest_exponent)
    query_shard = scaled_q * jnp.exp(rate_cum + before_block[:, None])
    dev_log = jnp.sum(block_total, axis=0)

    arriving_state = state_before_device(dev_log, dev_state)
    earlier_memory_share = jnp.einsum(
        "osyq,yqi->osyi", query_shard, arriving_state, precision=largest_exponent
    )
    mech_out = (within + earlier + earlier_memory_share).reshape(tok_rows, local_heads, DV)
    mech_out = (
        mech_out
        * lax.rsqrt(jnp.mean(mech_out * mech_out, axis=-1, keepdims=True) + eps)
        * head_norm_gain
    )
    mixed = (
        mech_out.reshape(tok_rows, local_heads * DV)
        * jax.nn.silu(emitted_switch_entries.astype(jnp.float32))
    ).astype(jnp.bfloat16)
    tp_count, tp_index = (lax.axis_size("tp"), lax.axis_index("tp"))
    share = tok_rows // tp_count
    mixed_all = jnp.concatenate(gather_tp(mixed), axis=1)
    attended = jnp.dot(mixed_all, out_full, preferred_element_type=jnp.float32)
    resid = residual_input_stream.astype(jnp.float32) + attended
    normed = row_norm(resid, feedforward_norm_gain)
    resid_own = lax.dynamic_slice_in_dim(resid, tp_index * share, share, 0)
    edge = normed[tok_rows - EDGE :]
    so_count, so_index = lax.axis_size("so"), lax.axis_index("so")
    first = lax.axis_index("si") == 0
    tail = jnp.where(first, from_behind(edge, SP, 1), from_behind(edge, "so", 1))
    width = 2 * gate_up_matrix.shape[0]
    other = pair_rows(normed)
    mine = jnp.concatenate([tail, normed], axis=0)
    gate_own = project(mine, gate_lines, width)
    value_own = project(mine, value_lines, width)
    gate_other = project(other, gate_lines, width)
    value_other = project(other, value_lines, width)

    def mix(up_own, up_other, taps):
        taps = my_half(taps)
        up_tail, up_own = up_own[:EDGE], up_own[EDGE:]
        own_end, other_end = up_own[tok_rows - EDGE :], up_other[tok_rows - EDGE :]
        own = depthwise(jnp.where(first, up_tail, other_end), up_own, taps)
        far = depthwise(jnp.where(first, own_end, up_tail), up_other, taps)
        return own, far

    gates = mix(gate_own, gate_other, gate_filter_taps)
    values = mix(value_own, value_other, value_filter_taps)
    hidden = [(jax.nn.silu(g) * v).astype(jnp.bfloat16) for g, v in zip(gates, values)]
    feed = jnp.zeros((share, resid.shape[1]), jnp.float32)
    for k, line in enumerate(down_lines):
        part = scatter_sum(*[jnp.dot(h, line, preferred_element_type=jnp.float32) for h in hidden])
        feed = lax.dynamic_update_slice_in_dim(feed, part, (so_index + k) % so_count * width, 1)
    return (resid_own + feed).astype(jnp.bfloat16)


def solution(mesh):
    sp, tp = mesh.shape["sp"], mesh.shape["tp"]
    split = Mesh(mesh.devices.reshape(sp // 2, 2, tp), ("so", "si", "tp"))
    placed = (
        P(SP, None),
        P(SP, "tp"),
        P(SP, "tp"),
        P(SP, "tp"),
        P(SP, "tp"),
        P(SP, "tp"),
        P(SP),
        P(),
        P("tp", None),
        P(),
        P(SP, "tp"),
        P(SP, "tp"),
        P(None, "tp"),
        P(None, "tp"),
        P("tp", SP),
    )
    return jax.shard_map(
        per_device, mesh=split, in_specs=placed, out_specs=P(("so", "si", "tp"), None), check_vma=False
    )
```

```python
import functools

import jax
import jax.numpy as jnp
from jax import lax
from jax.experimental import pallas as pl
from jax.experimental.pallas import tpu as pltpu
from jax.sharding import Mesh, PartitionSpec as P

DK = 64
DV = 128
CONV = 3
BLOCK = 64
EDGE = 16
SP = ("so", "si")


eps = 1e-06
retention_sharpness = 16.0


def from_behind(block, axis, distance):
    devices = range(lax.axis_size(axis))
    route = [(i - distance, i) for i in devices if i - distance in devices]
    return lax.ppermute(block, axis, route)


def to_blocks(tensor, local_heads, width):
    count = tensor.shape[0] // BLOCK
    return tensor.astype(jnp.float32).reshape(count, BLOCK, local_heads, width)


def row_norm(stream, gain):
    scaled = stream * lax.rsqrt(jnp.mean(stream * stream, axis=-1, keepdims=True) + eps)
    return (scaled * gain).astype(jnp.bfloat16)


def state_before_device(dev_log, dev_state):
    heads, channels, width = dev_state.shape
    lanes = heads * channels
    decay = jnp.pad(jnp.exp(dev_log).reshape(1, lanes), ((0, 0), (0, -lanes % width)))
    decay = decay.reshape(-1, width)
    packed = jnp.concatenate([dev_state.reshape(lanes, width), decay], axis=0)
    arriving = jnp.zeros_like(dev_state)
    after = jnp.ones((heads, channels), jnp.float32)
    for distance in range(1, lax.axis_size("so") * lax.axis_size("si")):
        got = from_behind(packed, SP, distance)
        arriving = arriving + after[..., None] * got[:lanes].reshape(dev_state.shape)
        after = after * got[lanes:].reshape(-1)[:lanes].reshape(after.shape)
    return arriving


def xor_route(axis, bit):
    return [(i, i ^ bit) for i in range(lax.axis_size(axis))]


def exchange(block, axis, bit):
    return lax.ppermute(block, axis, xor_route(axis, bit))


def gather_tp(block):
    count, me = lax.axis_size("tp"), lax.axis_index("tp")
    held = block[None]
    bit = count // 2
    while bit:
        other = exchange(held, "tp", bit)
        low = (me & bit) == 0
        held = jnp.stack([jnp.where(low, held, other), jnp.where(low, other, held)])
        held = held.reshape((-1,) + block.shape)
        bit //= 2
    bits = count.bit_length() - 1
    order = [sum(((t >> b) & 1) << (bits - 1 - b) for b in range(bits)) for t in range(count)]
    return [held[o] for o in order]


def swap_halves(block):
    first = lax.axis_index("si") == 0
    half = block.shape[0] // 2
    low, high = block[:half], block[half:]
    keep, give = jnp.where(first, low, high), jnp.where(first, high, low)
    got = exchange(give, "si", 1)
    return jnp.concatenate([jnp.where(first, keep, got), jnp.where(first, got, keep)], axis=1)


def line_gather(block):
    count, me = lax.axis_size("so"), lax.axis_index("so")
    if count != 4:
        whole = lax.all_gather(block, "so", axis=0)
        return [lax.dynamic_index_in_dim(whole, (me + k) % count, 0, False) for k in range(count)]
    across = lax.ppermute(block, "so", [(i, i ^ 2) for i in range(4)])
    above = lax.ppermute(block, "so", [(1, 0), (2, 1), (3, 2)])
    below = lax.ppermute(block, "so", [(0, 1), (1, 2), (2, 3)])
    far = lax.ppermute(across, "so", [(1, 0), (2, 3)])
    return [block, jnp.where(me == 3, far, above), across, jnp.where(me == 0, far, below)]


def pair_rows(normed):
    share = normed.shape[0] // 2
    mine = lax.axis_index("tp") % 2
    part = exchange(lax.dynamic_slice_in_dim(normed, mine * share, share, 0), "si", 1)
    other = exchange(part, "tp", 1)
    first = mine == 0
    return jnp.concatenate([jnp.where(first, part, other), jnp.where(first, other, part)], axis=0)


def project(rows, lines, width):
    count, me = lax.axis_size("so"), lax.axis_index("so")
    total = 0.0
    for k, line in enumerate(lines):
        part = lax.dynamic_slice_in_dim(rows, (me + k) % count * width, width, 1)
        total = total + lax.dot_general(
            part, line, (((1,), (1,)), ((), ())), preferred_element_type=jnp.float32
        )
    return total.astype(jnp.bfloat16)


def depthwise(before, body, taps):
    padded = jnp.concatenate([before, body], axis=0)
    start = padded.shape[0] - body.shape[0] - (CONV - 1)
    result = jnp.zeros(body.shape, jnp.float32)
    for offset in range(CONV):
        result = result + taps[offset].astype(jnp.float32)[None] * padded[
            start + offset : start + offset + body.shape[0]
        ].astype(jnp.float32)
    return result


def my_half(taps):
    half = taps.shape[1] // 2
    return jnp.where(lax.axis_index("si") == 0, taps[:, :half], taps[:, half:])


def halve(held, axis, bit):
    mine = (lax.axis_index(axis) // bit) % 2
    keep = lax.dynamic_index_in_dim(held, mine, 1, False)
    give = lax.dynamic_index_in_dim(held, 1 - mine, 1, False)
    got = exchange(give.astype(jnp.bfloat16), axis, bit)
    return keep.astype(jnp.float32) + got.astype(jnp.float32)


def scatter_sum(own, other):
    count = lax.axis_size("tp")
    share = own.shape[0] // count
    held = jnp.concatenate([own, other], axis=0)
    held = halve(held.reshape(count, 2, share, -1), "tp", 1)
    held = held.reshape(2, count // 2, share, -1)
    got = exchange(held[1].astype(jnp.bfloat16), "si", 1)
    held = held[0] + got.astype(jnp.float32)
    bit = 2
    while bit < count:
        held = halve(held.reshape((-1, 2) + held.shape[1:]), "tp", bit)
        bit *= 2
    return held[0]


def per_device(
    residual_input_stream,
    projected_queries,
    projected_keys,
    projected_values,
    emitted_switch_entries,
    retention_preactivations,
    additional_fading_amount,
    head_norm_gain,
    attention_output_weight,
    feedforward_norm_gain,
    gate_up_matrix,
    value_up_matrix,
    gate_filter_taps,
    value_filter_taps,
    down_projection_weight,
):
    largest_exponent = lax.Precision.HIGHEST
    tok_rows = residual_input_stream.shape[0]
    local_heads = projected_queries.shape[1] // DK
    gate_lines = line_gather(swap_halves(gate_up_matrix.T))
    value_lines = line_gather(swap_halves(value_up_matrix.T))
    down_lines = line_gather(swap_halves(down_projection_weight))
    out_full = jnp.concatenate(gather_tp(attention_output_weight), axis=0)
    retention_logarithm = (
        jax.nn.log_sigmoid(retention_preactivations.astype(jnp.float32)) / retention_sharpness
        + additional_fading_amount[:, None]
    )
    scaled_q = to_blocks(projected_queries, local_heads, DK) * DK ** (-0.5)
    key_heads = to_blocks(projected_keys, local_heads, DK)
    value_heads = to_blocks(projected_values, local_heads, DV)
    rate_cum = jnp.cumsum(to_blocks(retention_logarithm, local_heads, DK), axis=1)
    block_total = rate_cum[:, -1]
    before_block = jnp.cumsum(block_total, axis=0) - block_total
    q_decayed = scaled_q * jnp.exp(rate_cum)
    k_growth = key_heads * jnp.exp(-rate_cum)
    fading_through_finish = key_heads * jnp.exp(block_total[:, None] - rate_cum)
    lower = jnp.tril(jnp.ones((BLOCK, BLOCK), bool))
    scores = jnp.einsum("nihk,njhk->nhij", q_decayed, k_growth, precision=largest_exponent)
    scores = jnp.where(lower[None, None], scores, 0.0)
    within = jnp.einsum("nhij,njhv->nihv", scores, value_heads, precision=largest_exponent)
    increments = jnp.einsum(
        "nchk,nchv->nhkv", fading_through_finish, value_heads, precision=largest_exponent
    )

    count = block_total.shape[0]
    ends = before_block + block_total
    reached = jnp.concatenate([before_block, ends[-1:]], axis=0)
    earlier_block = jnp.arange(count)[None, :] < jnp.arange(count + 1)[:, None]
    fade = jnp.where(
        earlier_block[..., None, None],
        jnp.exp(jnp.minimum(reached[:, None] - ends[None], 0.0)),
        0.0,
    )
    states = jnp.sum(fade[..., None] * increments[None], axis=1)
    state_before, dev_state = states[:-1], states[-1]
    earlier = jnp.einsum("nchk,nhkv->nchv", q_decayed, state_before, precision=largest_exponent)
    query_shard = scaled_q * jnp.exp(rate_cum + before_block[:, None])
    dev_log = jnp.sum(block_total, axis=0)

    arriving_state = state_before_device(dev_log, dev_state)
    earlier_memory_share = jnp.einsum(
        "osyq,yqi->osyi", query_shard, arriving_state, precision=largest_exponent
    )
    mech_out = (within + earlier + earlier_memory_share).reshape(tok_rows, local_heads, DV)
    mech_out = (
        mech_out
        * lax.rsqrt(jnp.mean(mech_out * mech_out, axis=-1, keepdims=True) + eps)
        * head_norm_gain
    )
    mixed = (
        mech_out.reshape(tok_rows, local_heads * DV)
        * jax.nn.silu(emitted_switch_entries.astype(jnp.float32))
    ).astype(jnp.bfloat16)
    tp_count, tp_index = (lax.axis_size("tp"), lax.axis_index("tp"))
    share = tok_rows // tp_count
    mixed_all = jnp.concatenate(gather_tp(mixed), axis=1)
    attended = jnp.dot(mixed_all, out_full, preferred_element_type=jnp.float32)
    resid = residual_input_stream.astype(jnp.float32) + attended
    normed = row_norm(resid, feedforward_norm_gain)
    resid_own = lax.dynamic_slice_in_dim(resid, tp_index * share, share, 0)
    edge = normed[tok_rows - EDGE :]
    so_count, so_index = lax.axis_size("so"), lax.axis_index("so")
    first = lax.axis_index("si") == 0
    tail = jnp.where(first, from_behind(edge, SP, 1), from_behind(edge, "so", 1))
    width = 2 * gate_up_matrix.shape[0]
    other = pair_rows(normed)
    mine = jnp.concatenate([tail, normed], axis=0)
    gate_own = project(mine, gate_lines, width)
    value_own = project(mine, value_lines, width)
    gate_other = project(other, gate_lines, width)
    value_other = project(other, value_lines, width)

    def mix(up_own, up_other, taps):
        taps = my_half(taps)
        up_tail, up_own = up_own[:EDGE], up_own[EDGE:]
        own_end, other_end = up_own[tok_rows - EDGE :], up_other[tok_rows - EDGE :]
        own = depthwise(jnp.where(first, up_tail, other_end), up_own, taps)
        far = depthwise(jnp.where(first, own_end, up_tail), up_other, taps)
        return own, far

    gates = mix(gate_own, gate_other, gate_filter_taps)
    values = mix(value_own, value_other, value_filter_taps)
    hidden = [(jax.nn.silu(g) * v).astype(jnp.bfloat16) for g, v in zip(gates, values)]
    feed = jnp.zeros((share, resid.shape[1]), jnp.float32)
    for k, line in enumerate(down_lines):
        part = scatter_sum(*[jnp.dot(h, line, preferred_element_type=jnp.float32) for h in hidden])
        feed = lax.dynamic_update_slice_in_dim(feed, part, (so_index + k) % so_count * width, 1)
    return (resid_own + feed).astype(jnp.bfloat16)


def nt_dot(a, b, precision=None):
    return lax.dot_general(
        a, b, (((1,), (1,)), ((), ())), precision=precision, preferred_element_type=jnp.float32
    )


def layer_kernel(
    wsrc, osrc, q, k, v, gates, logr, res, hgain, fgain, taps,
    out,
    wbuf, obuf, mixbuf, rows, acc, hid, mech, qs, state, before, packed, got, arrived, resid,
    csend, crecv, ckeep, ysend, yrecv, ykeep, xsend, xrecv, xkeep,
    wrecv_sem, wsend_sem, orecv_sem, osend_sem, mrecv_sem, msend_sem, srecv_sem, ssend_sem,
    trecv_sem, tsend_sem, crecv_sem, csend_sem, yrecv_sem, ysend_sem, xrecv_sem, xsend_sem,
):
    highest = lax.Precision.HIGHEST
    s, t = lax.axis_index("sp"), lax.axis_index("tp")
    z, y, x, c = s // 2, s % 2, t // 2, t % 2
    sp_count, tp_count = lax.axis_size("sp"), lax.axis_size("tp")
    tok_rows, depth = q.shape[0], wsrc.shape[3]
    half = wsrc.shape[2]
    share = out.shape[0]
    wide = 2 * depth

    def copy(src, dst, send, recv, zz, yy, tt):
        return pltpu.make_async_remote_copy(
            src_ref=src, dst_ref=dst, send_sem=send, recv_sem=recv,
            device_id=(zz * 2 + yy, tt), device_id_type=pl.DeviceIdType.MESH,
        )

    def wait_recv(ref, send, recv):
        copy(ref, ref, send, recv, z, y, t).wait_recv()

    def wait_send(ref, send, recv):
        copy(ref, ref, send, recv, z, y, t).wait_send()

    def cols(index, width):
        return pl.ds(pl.multiple_of(index * width, width), width)

    t_core, t_chip, t_diag = x * 2 + 1 - c, (1 - x) * 2 + c, (1 - x) * 2 + 1 - c

    barrier = pltpu.get_barrier_semaphore()

    @pl.loop(0, sp_count * tp_count)
    def _(i):
        pl.semaphore_signal(
            barrier, inc=1, device_id=(i // tp_count, i % tp_count), device_id_type=pl.DeviceIdType.MESH
        )

    pl.semaphore_wait(barrier, sp_count * tp_count)

    def block(m, zz, h):
        return wbuf.at[m, zz, :, cols(h, depth)]

    def local_copy(m):
        return pltpu.make_async_copy(wsrc.at[m, y], block(m, z, y), wrecv_sem.at[m, z, y])

    def hop(m):
        return copy(wsrc.at[m, 1 - y], block(m, z, y), wsend_sem.at[m, 0, 4], wrecv_sem.at[m, z, y], z, 1 - y, t)

    far = (z + 2) % 4

    def line_copies(m, own):
        h = y if own else 1 - y
        src = wsrc.at[m, y] if own else block(m, z, h)
        slot = 0 if own else 1
        dests = ((far, None), (z + 1, z < 3), (z - 1, z > 0))
        return [
            (copy(src, block(m, z, h), wsend_sem.at[m, slot, i], wrecv_sem.at[m, z, h], dest, y, t), cond)
            for i, (dest, cond) in enumerate(dests)
        ]

    def each(copies, act):
        for one, cond in copies:
            if cond is None:
                act(one)
            else:
                pl.when(cond)(functools.partial(act, one))

    def start(one):
        one.start()

    def send_own(m):
        each(line_copies(m, True), start)

    def send_other(m):
        wait_recv(block(m, z, 1 - y), wsend_sem.at[m, 0, 4], wrecv_sem.at[m, z, 1 - y])
        each(line_copies(m, False), start)

    inner = (z > 0) & (z < 3)

    def relay(m, h):
        return copy(
            block(m, far, h), block(m, far, h), wsend_sem.at[m, h, 3], wrecv_sem.at[m, far, h], 3 * (z - 1), y, t
        )

    def relays(m):
        @pl.when(inner)
        def _():
            for h in range(2):
                wait_recv(block(m, far, h), wsend_sem.at[m, h, 3], wrecv_sem.at[m, far, h])
                relay(m, h).start()

    def tp_copies(src, buf, send, recv):
        return (
            copy(src, buf.at[t], send.at[0], recv.at[t], z, y, t_core),
            copy(src, buf.at[t], send.at[1], recv.at[t], z, y, t_chip),
        )

    def tp_relay(buf, send, recv):
        return copy(buf.at[t_chip], buf.at[t_chip], send.at[2], recv.at[t_chip], z, y, t_core)

    def tp_pass_on(buf, send, recv):
        wait_recv(buf.at[t_chip], send.at[2], recv.at[t_chip])
        tp_relay(buf, send, recv).start()

    def tp_arrive(buf, send, recv):
        wait_recv(buf.at[t_core], send.at[0], recv.at[t_core])
        wait_recv(buf.at[t_diag], send.at[0], recv.at[t_diag])

    for m in range(3):
        hop(m).start()
        if m == 0:
            send_own(0)
    for m in range(3):
        local_copy(m).start()
    own_out = pltpu.make_async_copy(osrc, obuf.at[t], orecv_sem.at[t])
    own_out.start()
    for one in tp_copies(osrc, obuf, osend_sem, orecv_sem):
        one.start()

    scale = DK ** (-0.5)
    key_lanes = q.shape[1]
    val_lanes = v.shape[1]
    lane_head = lax.broadcasted_iota(jnp.int32, (BLOCK, key_lanes), 1) // DK
    heads = key_lanes // DK
    low = lax.broadcasted_iota(jnp.int32, (BLOCK, BLOCK), 0) >= lax.broadcasted_iota(jnp.int32, (BLOCK, BLOCK), 1)
    low_ones = low.astype(jnp.float32)
    same_head = (
        lax.broadcasted_iota(jnp.int32, (val_lanes, key_lanes), 0) // DV
        == lax.broadcasted_iota(jnp.int32, (val_lanes, key_lanes), 1) // DK
    )
    state[...] = jnp.zeros_like(state)
    before[...] = jnp.zeros_like(before)

    def attend_block(i):
        at = pl.ds(pl.multiple_of(i * BLOCK, BLOCK), BLOCK)
        rate = logr[at, :]
        cum = jnp.dot(low_ones, rate, precision=highest, preferred_element_type=jnp.float32)
        total = cum[BLOCK - 1 :, :]
        ahead = before[0:1, :]
        q_decayed = q[at, :].astype(jnp.float32) * scale * jnp.exp(cum)
        qs[at, :] = q[at, :].astype(jnp.float32) * scale * jnp.exp(cum + ahead)
        keys = k[at, :].astype(jnp.float32)
        grown = keys * jnp.exp(-cum)
        ending = keys * jnp.exp(total - cum)
        values = v[at, :].astype(jnp.float32)
        inside = []
        for h in range(heads):
            mine = lane_head == h
            scores = nt_dot(jnp.where(mine, q_decayed, 0.0), jnp.where(mine, grown, 0.0), highest)
            scores = jnp.where(low, scores, 0.0)
            inside.append(
                jnp.dot(
                    scores, values[:, h * DV : (h + 1) * DV], precision=highest, preferred_element_type=jnp.float32
                )
            )
        old = state[...]
        mech[at, :] = jnp.concatenate(inside, axis=1) + nt_dot(q_decayed, old, highest)
        step = lax.dot_general(
            values, ending, (((0,), (0,)), ((), ())), precision=highest, preferred_element_type=jnp.float32
        )
        state[...] = old * jnp.exp(total) + jnp.where(same_head, step, 0.0)
        before[...] = jnp.broadcast_to(ahead + total, before.shape)

    blocks = tok_rows // BLOCK
    pl.loop(0, blocks // 2)(attend_block)
    send_other(0)
    pl.loop(blocks // 2, blocks)(attend_block)

    lanes = packed.shape[1]
    whole = state[0:DV, :]
    for h in range(1, heads):
        whole = whole + state[h * DV : (h + 1) * DV, :]
    packed[0:DV, :] = whole
    packed[DV:, :] = jnp.exp(before[...])

    def state_copy(d):
        to = s + d
        return copy(packed, got.at[d], ssend_sem.at[d], srecv_sem.at[d], to // 2, to % 2, t)

    for d in range(1, 8):
        pl.when(s + d < sp_count)(functools.partial(start, state_copy(d)))
    tp_pass_on(obuf, osend_sem, orecv_sem)
    send_own(1)
    send_other(1)
    arrived[...] = jnp.zeros_like(arrived)
    before[...] = jnp.ones_like(before)
    for d in range(1, 8):
        @pl.when(s >= d)
        def _(d=d):
            wait_recv(got.at[d], ssend_sem.at[d], srecv_sem.at[d])
            arrived[...] += before[0:1, :] * got[d, 0:DV, :]
            before[...] = before[...] * got[d, DV:, :]

    lane_wide = lax.broadcasted_iota(jnp.int32, (share, key_lanes), 1) // DK
    lane_state = lax.broadcasted_iota(jnp.int32, (DV, key_lanes), 1) // DK

    @pl.loop(0, tok_rows // share)
    def _(i):
        at = pl.ds(pl.multiple_of(i * share, share), share)
        for h in range(heads):
            part = pl.ds(h * DV, DV)
            extra = nt_dot(
                jnp.where(lane_wide == h, qs[at, :], 0.0), jnp.where(lane_state == h, arrived[...], 0.0), highest
            )
            o = mech[at, part] + extra
            o = o * lax.rsqrt(jnp.mean(o * o, axis=-1, keepdims=True) + eps) * hgain[...]
            gate = gates[at, part].astype(jnp.float32)
            mixbuf[t, at, part] = (o * (gate * jax.nn.sigmoid(gate))).astype(jnp.bfloat16)

    for one in tp_copies(mixbuf.at[t], mixbuf, msend_sem, mrecv_sem):
        one.start()
    relays(0)
    own_out.wait()
    tp_arrive(obuf, osend_sem, orecv_sem)
    tp_pass_on(mixbuf, msend_sem, mrecv_sem)
    tp_arrive(mixbuf, msend_sem, mrecv_sem)

    def tile_at(yy, tile):
        return pl.ds(pl.multiple_of(EDGE + yy * tok_rows + tile * share, EDGE), share)

    def tile_copy(i, tile):
        ref = rows.at[tile_at(y, tile), :]
        return copy(ref, ref, tsend_sem.at[i], trecv_sem.at[tile], z, 1 - y, t)

    @pl.loop(0, tp_count)
    def _(i):
        tile = (2 * c + i) % tp_count
        at = pl.ds(pl.multiple_of(tile * share, share), share)
        total = res[at, :].astype(jnp.float32)
        for part in range(tp_count):
            total = total + jnp.dot(mixbuf[part, at, :], obuf[part], preferred_element_type=jnp.float32)
        scaled = total * lax.rsqrt(jnp.mean(total * total, axis=-1, keepdims=True) + eps)
        rows[tile_at(y, tile), :] = (scaled * fgain[...]).astype(jnp.bfloat16)

        @pl.when(tile == t)
        def _():
            resid[...] = total

        @pl.when(i < 2)
        def _():
            tile_copy(i, tile).start()

    last = rows.at[pl.ds(EDGE + 2 * tok_rows - EDGE, EDGE), :]
    head = rows.at[pl.ds(0, EDGE), :]

    def edge_copy(yy):
        return copy(last, head, tsend_sem.at[4 + yy], trecv_sem.at[tp_count], z + 1, yy, t)

    @pl.when((y == 1) & (z < 3))
    def _():
        edge_copy(0).start()
        edge_copy(1).start()

    @pl.when(z == 0)
    def _():
        rows[0:EDGE, :] = jnp.zeros((EDGE, rows.shape[1]), rows.dtype)

    send_own(2)
    send_other(2)

    def pass_copy(i):
        ref = rows.at[tile_at(1 - y, 2 * c + i), :]
        return copy(ref, ref, tsend_sem.at[2 + i], trecv_sem.at[2 * c + i], z, y, t_core)

    towards = jnp.where(z < 2, 1, 3)

    def source(step):
        return (z + step * towards) % 4

    def weights_here(m, step):
        zk = source(step)
        if step == 0:
            local_copy(m).wait()
        else:
            @pl.when(jnp.logical_not(inner & (zk == far)))
            def _():
                for h in range(2):
                    wait_recv(block(m, zk, h), wsend_sem.at[m, h, 3], wrecv_sem.at[m, zk, h])

    def project(m, step, first_row, size, tiles):
        zk = source(step)

        def tile(i):
            at = pl.ds(pl.multiple_of(first_row + i * size, EDGE), size)
            part = nt_dot(rows[at, cols(zk, wide)], wbuf[m, zk])
            if step == 0:
                acc[m, at, :] = part
            else:
                acc[m, at, :] += part

        if tiles == 1:
            tile(0)
        else:
            pl.loop(0, tiles)(tile)

    tall = tok_rows // 2
    for m in range(2):
        for step in range(4):
            weights_here(m, step)
            project(m, step, EDGE + y * tok_rows, tall, 2)
        if m == 0:
            for i in range(2):
                ref = rows.at[tile_at(1 - y, 2 * c + i), :]
                wait_recv(ref, tsend_sem.at[2 + i], trecv_sem.at[2 * c + i])
                pass_copy(i).start()
            relays(1)
    for i in range(2):
        ref = rows.at[tile_at(1 - y, 2 * (1 - c) + i), :]
        wait_recv(ref, tsend_sem.at[2 + i], trecv_sem.at[2 * (1 - c) + i])

    @pl.when(z > 0)
    def _():
        wait_recv(head, tsend_sem.at[4], trecv_sem.at[tp_count])

    for m in range(2):
        for step in range(4):
            project(m, step, EDGE + (1 - y) * tok_rows, tall, 2)
            project(m, step, 0, EDGE, 1)

    @pl.loop(0, 2 * tok_rows // share)
    def _(i):
        at = pl.ds(pl.multiple_of(i * share, EDGE), share + EDGE)

        def mix(m):
            up = acc[m, at, :].astype(jnp.bfloat16).astype(jnp.float32)
            total = jnp.zeros_like(up)
            for j in range(CONV):
                back = CONV - 1 - j
                moved = up if back == 0 else pltpu.roll(up, back, 0)
                total = total + taps[m * CONV + j : m * CONV + j + 1, :] * moved
            return total[EDGE:, :]

        gate = mix(0)
        to = pl.ds(pl.multiple_of(i * share, share), share)
        hid[to, :] = (gate * jax.nn.sigmoid(gate) * mix(1)).astype(jnp.bfloat16)

    relays(2)

    count = 8

    def down(b):
        step, h = b // 2, b % 2
        if h == 0:
            weights_here(2, step)
        weight = wbuf[2, source(step), :, h * depth : (h + 1) * depth]

        @pl.loop(0, tp_count)
        def _(j):
            give = pl.ds(pl.multiple_of((2 * j + 1 - c) * share, share), share)
            keep = pl.ds(pl.multiple_of((2 * j + c) * share, share), share)
            csend[b, j] = jnp.dot(hid[give, :], weight, preferred_element_type=jnp.float32).astype(jnp.bfloat16)
            ckeep[b % 2, j] = jnp.dot(hid[keep, :], weight, preferred_element_type=jnp.float32)

        c_copy(b).start()

    def c_copy(b):
        return copy(csend.at[b], crecv.at[b], csend_sem.at[b], crecv_sem.at[b], z, y, t_core)

    def y_copy(b):
        return copy(ysend.at[b], yrecv.at[b], ysend_sem.at[b], yrecv_sem.at[b], z, 1 - y, t)

    def x_copy(b):
        return copy(xsend.at[b], xrecv.at[b], xsend_sem.at[b], xrecv_sem.at[b], z, y, t_chip)

    def over_c(b):
        c_copy(b).wait()
        for xx in range(2):
            j = (1 - y) * 2 + xx
            ysend[b, xx] = (ckeep[b % 2, j] + crecv[b, j].astype(jnp.float32)).astype(jnp.bfloat16)
        y_copy(b).start()
        for xx in range(2):
            j = y * 2 + xx
            ykeep[b % 2, xx] = ckeep[b % 2, j] + crecv[b, j].astype(jnp.float32)

    def over_y(b):
        y_copy(b).wait()
        xsend[b] = (ykeep[b % 2, 1 - x] + yrecv[b, 1 - x].astype(jnp.float32)).astype(jnp.bfloat16)
        x_copy(b).start()
        xkeep[b % 2] = ykeep[b % 2, x] + yrecv[b, x].astype(jnp.float32)

    def over_x(b):
        x_copy(b).wait()
        at = pl.ds(pl.multiple_of(source(b // 2) * wide + b % 2 * depth, depth), depth)
        total = resid[:, at] + (xkeep[b % 2] + xrecv[b].astype(jnp.float32))
        out[:, at] = total.astype(out.dtype)

    for b in range(count + 3):
        if 0 <= b - 3:
            over_x(b - 3)
        if 0 <= b - 2 < count:
            over_y(b - 2)
        if 0 <= b - 1 < count:
            over_c(b - 1)
        if b < count:
            down(b)

    def finish(one):
        one.wait_send()

    for m in range(3):
        finish(hop(m))
        each(line_copies(m, True), finish)
        each(line_copies(m, False), finish)

        @pl.when(inner)
        def _(m=m):
            for h in range(2):
                finish(relay(m, h))
    for src, buf, send, recv in (
        (osrc, obuf, osend_sem, orecv_sem),
        (mixbuf.at[t], mixbuf, msend_sem, mrecv_sem),
    ):
        for one in tp_copies(src, buf, send, recv):
            finish(one)
        finish(tp_relay(buf, send, recv))
    for d in range(1, 8):
        pl.when(s + d < sp_count)(functools.partial(finish, state_copy(d)))
    for i in range(2):
        finish(tile_copy(i, 2 * c + i))
        finish(pass_copy(i))

    @pl.when((y == 1) & (z < 3))
    def _():
        finish(edge_copy(0))
        finish(edge_copy(1))


def fused_layer(
    residual_input_stream,
    projected_queries,
    projected_keys,
    projected_values,
    emitted_switch_entries,
    retention_preactivations,
    additional_fading_amount,
    head_norm_gain,
    attention_output_weight,
    feedforward_norm_gain,
    gate_up_matrix,
    value_up_matrix,
    gate_filter_taps,
    value_filter_taps,
    down_projection_weight,
):
    tok_rows, width = residual_input_stream.shape
    keys, vals = projected_queries.shape[1], projected_values.shape[1]
    depth, units = gate_up_matrix.shape
    half, tp = units // 2, lax.axis_size("tp")
    share = tok_rows // tp
    first = lax.axis_index("sp") % 2 == 0
    weights = jnp.stack([gate_up_matrix.T, value_up_matrix.T, down_projection_weight])
    weights = weights.reshape(3, 2, half, depth)
    rates = (
        jax.nn.log_sigmoid(retention_preactivations.astype(jnp.float32)) / retention_sharpness
        + additional_fading_amount[:, None]
    )
    taps = jnp.concatenate([gate_filter_taps, value_filter_taps], axis=0).astype(jnp.float32)
    taps = jnp.where(first, taps[:, :half], taps[:, half:])
    bf16, f32, dma = jnp.bfloat16, jnp.float32, pltpu.SemaphoreType.DMA
    hbm, vmem = pl.BlockSpec(memory_space=pl.ANY), pl.BlockSpec(memory_space=pltpu.VMEM)
    scratch = [
        pltpu.VMEM((3, 4, half, 2 * depth), bf16),
        pltpu.VMEM((tp, vals, width), bf16),
        pltpu.VMEM((tp, tok_rows, vals), bf16),
        pltpu.VMEM((EDGE + 2 * tok_rows, width), bf16),
        pltpu.VMEM((2, EDGE + 2 * tok_rows, half), f32),
        pltpu.VMEM((2 * tok_rows, half), bf16),
        pltpu.VMEM((tok_rows, vals), f32),
        pltpu.VMEM((tok_rows, keys), f32),
        pltpu.VMEM((vals, keys), f32),
        pltpu.VMEM((8, keys), f32),
        pltpu.VMEM((DV + 8, keys), f32),
        pltpu.VMEM((8, DV + 8, keys), f32),
        pltpu.VMEM((DV, keys), f32),
        pltpu.VMEM((share, width), f32),
        pltpu.VMEM((8, 4, share, depth), bf16),
        pltpu.VMEM((8, 4, share, depth), bf16),
        pltpu.VMEM((2, 4, share, depth), f32),
        pltpu.VMEM((8, 2, share, depth), bf16),
        pltpu.VMEM((8, 2, share, depth), bf16),
        pltpu.VMEM((2, 2, share, depth), f32),
        pltpu.VMEM((8, share, depth), bf16),
        pltpu.VMEM((8, share, depth), bf16),
        pltpu.VMEM((2, share, depth), f32),
        dma((3, 4, 2)), dma((3, 2, 5)), dma((tp,)), dma((3,)), dma((tp,)), dma((3,)), dma((8,)), dma((8,)),
        dma((tp + 1,)), dma((6,)), dma((8,)), dma((8,)), dma((8,)), dma((8,)), dma((8,)), dma((8,)),
    ]
    return pl.pallas_call(
        layer_kernel,
        name="layer",
        out_shape=jax.ShapeDtypeStruct((share, width), bf16),
        in_specs=[hbm, hbm] + [vmem] * 9,
        out_specs=vmem,
        scratch_shapes=scratch,
        compiler_params=pltpu.CompilerParams(
            collective_id=0, has_side_effects=True, vmem_limit_bytes=67043328
        ),
    )(
        weights, attention_output_weight, projected_queries, projected_keys, projected_values,
        emitted_switch_entries, rates, residual_input_stream, head_norm_gain[None], feedforward_norm_gain[None], taps,
    )


def specs(rows):
    return (
            P(rows, None),
            P(rows, "tp"),
            P(rows, "tp"),
            P(rows, "tp"),
            P(rows, "tp"),
            P(rows, "tp"),
            P(rows),
            P(),
            P("tp", None),
            P(),
            P(rows, "tp"),
            P(rows, "tp"),
            P(None, "tp"),
            P(None, "tp"),
            P("tp", rows),
    )


def solution(mesh):
    sp, tp = mesh.shape["sp"], mesh.shape["tp"]
    if sp == 8 and tp == 4:
        return jax.shard_map(
            fused_layer,
            mesh=mesh,
            in_specs=specs("sp"),
            out_specs=P(("sp", "tp"), None),
            check_vma=False,
        )
    split = Mesh(mesh.devices.reshape(sp // 2, 2, tp), ("so", "si", "tp"))
    return jax.shard_map(
        per_device, mesh=split, in_specs=specs(SP), out_specs=P(("so", "si", "tp"), None), check_vma=False
    )
```

```python
import functools

import jax
import jax.numpy as jnp
from jax import lax
from jax.experimental import pallas as pl
from jax.experimental.pallas import tpu as pltpu
from jax.sharding import Mesh, PartitionSpec as P

DK = 64
DV = 128
CONV = 3
BLOCK = 64
EDGE = 16
SP = ("so", "si")


eps = 1e-06
retention_sharpness = 16.0


def from_behind(block, axis, distance):
    devices = range(lax.axis_size(axis))
    route = [(i - distance, i) for i in devices if i - distance in devices]
    return lax.ppermute(block, axis, route)


def to_blocks(tensor, local_heads, width):
    count = tensor.shape[0] // BLOCK
    return tensor.astype(jnp.float32).reshape(count, BLOCK, local_heads, width)


def row_norm(stream, gain):
    scaled = stream * lax.rsqrt(jnp.mean(stream * stream, axis=-1, keepdims=True) + eps)
    return (scaled * gain).astype(jnp.bfloat16)


def state_before_device(dev_log, dev_state):
    heads, channels, width = dev_state.shape
    lanes = heads * channels
    decay = jnp.pad(jnp.exp(dev_log).reshape(1, lanes), ((0, 0), (0, -lanes % width)))
    decay = decay.reshape(-1, width)
    packed = jnp.concatenate([dev_state.reshape(lanes, width), decay], axis=0)
    arriving = jnp.zeros_like(dev_state)
    after = jnp.ones((heads, channels), jnp.float32)
    for distance in range(1, lax.axis_size("so") * lax.axis_size("si")):
        got = from_behind(packed, SP, distance)
        arriving = arriving + after[..., None] * got[:lanes].reshape(dev_state.shape)
        after = after * got[lanes:].reshape(-1)[:lanes].reshape(after.shape)
    return arriving


def xor_route(axis, bit):
    return [(i, i ^ bit) for i in range(lax.axis_size(axis))]


def exchange(block, axis, bit):
    return lax.ppermute(block, axis, xor_route(axis, bit))


def gather_tp(block):
    count, me = lax.axis_size("tp"), lax.axis_index("tp")
    held = block[None]
    bit = count // 2
    while bit:
        other = exchange(held, "tp", bit)
        low = (me & bit) == 0
        held = jnp.stack([jnp.where(low, held, other), jnp.where(low, other, held)])
        held = held.reshape((-1,) + block.shape)
        bit //= 2
    bits = count.bit_length() - 1
    order = [sum(((t >> b) & 1) << (bits - 1 - b) for b in range(bits)) for t in range(count)]
    return [held[o] for o in order]


def swap_halves(block):
    first = lax.axis_index("si") == 0
    half = block.shape[0] // 2
    low, high = block[:half], block[half:]
    keep, give = jnp.where(first, low, high), jnp.where(first, high, low)
    got = exchange(give, "si", 1)
    return jnp.concatenate([jnp.where(first, keep, got), jnp.where(first, got, keep)], axis=1)


def line_gather(block):
    count, me = lax.axis_size("so"), lax.axis_index("so")
    if count != 4:
        whole = lax.all_gather(block, "so", axis=0)
        return [lax.dynamic_index_in_dim(whole, (me + k) % count, 0, False) for k in range(count)]
    across = lax.ppermute(block, "so", [(i, i ^ 2) for i in range(4)])
    above = lax.ppermute(block, "so", [(1, 0), (2, 1), (3, 2)])
    below = lax.ppermute(block, "so", [(0, 1), (1, 2), (2, 3)])
    far = lax.ppermute(across, "so", [(1, 0), (2, 3)])
    return [block, jnp.where(me == 3, far, above), across, jnp.where(me == 0, far, below)]


def pair_rows(normed):
    share = normed.shape[0] // 2
    mine = lax.axis_index("tp") % 2
    part = exchange(lax.dynamic_slice_in_dim(normed, mine * share, share, 0), "si", 1)
    other = exchange(part, "tp", 1)
    first = mine == 0
    return jnp.concatenate([jnp.where(first, part, other), jnp.where(first, other, part)], axis=0)


def project(rows, lines, width):
    count, me = lax.axis_size("so"), lax.axis_index("so")
    total = 0.0
    for k, line in enumerate(lines):
        part = lax.dynamic_slice_in_dim(rows, (me + k) % count * width, width, 1)
        total = total + lax.dot_general(
            part, line, (((1,), (1,)), ((), ())), preferred_element_type=jnp.float32
        )
    return total.astype(jnp.bfloat16)


def depthwise(before, body, taps):
    padded = jnp.concatenate([before, body], axis=0)
    start = padded.shape[0] - body.shape[0] - (CONV - 1)
    result = jnp.zeros(body.shape, jnp.float32)
    for offset in range(CONV):
        result = result + taps[offset].astype(jnp.float32)[None] * padded[
            start + offset : start + offset + body.shape[0]
        ].astype(jnp.float32)
    return result


def my_half(taps):
    half = taps.shape[1] // 2
    return jnp.where(lax.axis_index("si") == 0, taps[:, :half], taps[:, half:])


def halve(held, axis, bit):
    mine = (lax.axis_index(axis) // bit) % 2
    keep = lax.dynamic_index_in_dim(held, mine, 1, False)
    give = lax.dynamic_index_in_dim(held, 1 - mine, 1, False)
    got = exchange(give.astype(jnp.bfloat16), axis, bit)
    return keep.astype(jnp.float32) + got.astype(jnp.float32)


def scatter_sum(own, other):
    count = lax.axis_size("tp")
    share = own.shape[0] // count
    held = jnp.concatenate([own, other], axis=0)
    held = halve(held.reshape(count, 2, share, -1), "tp", 1)
    held = held.reshape(2, count // 2, share, -1)
    got = exchange(held[1].astype(jnp.bfloat16), "si", 1)
    held = held[0] + got.astype(jnp.float32)
    bit = 2
    while bit < count:
        held = halve(held.reshape((-1, 2) + held.shape[1:]), "tp", bit)
        bit *= 2
    return held[0]


def per_device(
    residual_input_stream,
    projected_queries,
    projected_keys,
    projected_values,
    emitted_switch_entries,
    retention_preactivations,
    additional_fading_amount,
    head_norm_gain,
    attention_output_weight,
    feedforward_norm_gain,
    gate_up_matrix,
    value_up_matrix,
    gate_filter_taps,
    value_filter_taps,
    down_projection_weight,
):
    largest_exponent = lax.Precision.HIGHEST
    tok_rows = residual_input_stream.shape[0]
    local_heads = projected_queries.shape[1] // DK
    gate_lines = line_gather(swap_halves(gate_up_matrix.T))
    value_lines = line_gather(swap_halves(value_up_matrix.T))
    down_lines = line_gather(swap_halves(down_projection_weight))
    out_full = jnp.concatenate(gather_tp(attention_output_weight), axis=0)
    retention_logarithm = (
        jax.nn.log_sigmoid(retention_preactivations.astype(jnp.float32)) / retention_sharpness
        + additional_fading_amount[:, None]
    )
    scaled_q = to_blocks(projected_queries, local_heads, DK) * DK ** (-0.5)
    key_heads = to_blocks(projected_keys, local_heads, DK)
    value_heads = to_blocks(projected_values, local_heads, DV)
    rate_cum = jnp.cumsum(to_blocks(retention_logarithm, local_heads, DK), axis=1)
    block_total = rate_cum[:, -1]
    before_block = jnp.cumsum(block_total, axis=0) - block_total
    q_decayed = scaled_q * jnp.exp(rate_cum)
    k_growth = key_heads * jnp.exp(-rate_cum)
    fading_through_finish = key_heads * jnp.exp(block_total[:, None] - rate_cum)
    lower = jnp.tril(jnp.ones((BLOCK, BLOCK), bool))
    scores = jnp.einsum("nihk,njhk->nhij", q_decayed, k_growth, precision=largest_exponent)
    scores = jnp.where(lower[None, None], scores, 0.0)
    within = jnp.einsum("nhij,njhv->nihv", scores, value_heads, precision=largest_exponent)
    increments = jnp.einsum(
        "nchk,nchv->nhkv", fading_through_finish, value_heads, precision=largest_exponent
    )

    count = block_total.shape[0]
    ends = before_block + block_total
    reached = jnp.concatenate([before_block, ends[-1:]], axis=0)
    earlier_block = jnp.arange(count)[None, :] < jnp.arange(count + 1)[:, None]
    fade = jnp.where(
        earlier_block[..., None, None],
        jnp.exp(jnp.minimum(reached[:, None] - ends[None], 0.0)),
        0.0,
    )
    states = jnp.sum(fade[..., None] * increments[None], axis=1)
    state_before, dev_state = states[:-1], states[-1]
    earlier = jnp.einsum("nchk,nhkv->nchv", q_decayed, state_before, precision=largest_exponent)
    query_shard = scaled_q * jnp.exp(rate_cum + before_block[:, None])
    dev_log = jnp.sum(block_total, axis=0)

    arriving_state = state_before_device(dev_log, dev_state)
    earlier_memory_share = jnp.einsum(
        "osyq,yqi->osyi", query_shard, arriving_state, precision=largest_exponent
    )
    mech_out = (within + earlier + earlier_memory_share).reshape(tok_rows, local_heads, DV)
    mech_out = (
        mech_out
        * lax.rsqrt(jnp.mean(mech_out * mech_out, axis=-1, keepdims=True) + eps)
        * head_norm_gain
    )
    mixed = (
        mech_out.reshape(tok_rows, local_heads * DV)
        * jax.nn.silu(emitted_switch_entries.astype(jnp.float32))
    ).astype(jnp.bfloat16)
    tp_count, tp_index = (lax.axis_size("tp"), lax.axis_index("tp"))
    share = tok_rows // tp_count
    mixed_all = jnp.concatenate(gather_tp(mixed), axis=1)
    attended = jnp.dot(mixed_all, out_full, preferred_element_type=jnp.float32)
    resid = residual_input_stream.astype(jnp.float32) + attended
    normed = row_norm(resid, feedforward_norm_gain)
    resid_own = lax.dynamic_slice_in_dim(resid, tp_index * share, share, 0)
    edge = normed[tok_rows - EDGE :]
    so_count, so_index = lax.axis_size("so"), lax.axis_index("so")
    first = lax.axis_index("si") == 0
    tail = jnp.where(first, from_behind(edge, SP, 1), from_behind(edge, "so", 1))
    width = 2 * gate_up_matrix.shape[0]
    other = pair_rows(normed)
    mine = jnp.concatenate([tail, normed], axis=0)
    gate_own = project(mine, gate_lines, width)
    value_own = project(mine, value_lines, width)
    gate_other = project(other, gate_lines, width)
    value_other = project(other, value_lines, width)

    def mix(up_own, up_other, taps):
        taps = my_half(taps)
        up_tail, up_own = up_own[:EDGE], up_own[EDGE:]
        own_end, other_end = up_own[tok_rows - EDGE :], up_other[tok_rows - EDGE :]
        own = depthwise(jnp.where(first, up_tail, other_end), up_own, taps)
        far = depthwise(jnp.where(first, own_end, up_tail), up_other, taps)
        return own, far

    gates = mix(gate_own, gate_other, gate_filter_taps)
    values = mix(value_own, value_other, value_filter_taps)
    hidden = [(jax.nn.silu(g) * v).astype(jnp.bfloat16) for g, v in zip(gates, values)]
    feed = jnp.zeros((share, resid.shape[1]), jnp.float32)
    for k, line in enumerate(down_lines):
        part = scatter_sum(*[jnp.dot(h, line, preferred_element_type=jnp.float32) for h in hidden])
        feed = lax.dynamic_update_slice_in_dim(feed, part, (so_index + k) % so_count * width, 1)
    return (resid_own + feed).astype(jnp.bfloat16)


def nt_dot(a, b, precision=None):
    return lax.dot_general(
        a, b, (((1,), (1,)), ((), ())), precision=precision, preferred_element_type=jnp.float32
    )


def layer_kernel(
    gate_in, value_in, down_in, osrc, q, k, v, gates, logr, res, hgain, fgain, gate_taps, value_taps,
    out,
    wsrc, taps, wbuf, obuf, mixbuf, rows, acc, hid, mech, qs, state, before, packed, joined, got, arrived, resid,
    csend, crecv, ckeep, ysend, yrecv, ykeep, xsend, xrecv, xkeep,
    wrecv_sem, wsend_sem, orecv_sem, osend_sem, mrecv_sem, msend_sem, srecv_sem, ssend_sem,
    trecv_sem, tsend_sem, crecv_sem, csend_sem, yrecv_sem, ysend_sem, xrecv_sem, xsend_sem,
):
    highest = lax.Precision.HIGHEST
    s, t = lax.axis_index("sp"), lax.axis_index("tp")
    z, y, x, c = s // 2, s % 2, t // 2, t % 2
    sp_count, tp_count = lax.axis_size("sp"), lax.axis_size("tp")
    tok_rows, (units, depth) = q.shape[0], down_in.shape
    half = units // 2
    share = out.shape[0]
    wide = 2 * depth

    def copy(src, dst, send, recv, zz, yy, tt):
        return pltpu.make_async_remote_copy(
            src_ref=src, dst_ref=dst, send_sem=send, recv_sem=recv,
            device_id=(zz * 2 + yy, tt), device_id_type=pl.DeviceIdType.MESH,
        )

    def wait_recv(ref, send, recv):
        copy(ref, ref, send, recv, z, y, t).wait_recv()

    def wait_send(ref, send, recv):
        copy(ref, ref, send, recv, z, y, t).wait_send()

    def cols(index, width):
        return pl.ds(pl.multiple_of(index * width, width), width)

    t_core, t_chip, t_diag = x * 2 + 1 - c, (1 - x) * 2 + c, (1 - x) * 2 + 1 - c

    wsrc[0] = jnp.transpose(gate_in[...])
    first = y == 0
    for m, given in enumerate((gate_taps, value_taps)):
        both = given[...].astype(jnp.float32)
        taps[m * CONV : (m + 1) * CONV, :] = jnp.where(first, both[:, :half], both[:, half:])

    barrier = pltpu.get_barrier_semaphore()

    @pl.loop(0, sp_count * tp_count)
    def _(i):
        pl.semaphore_signal(
            barrier, inc=1, device_id=(i // tp_count, i % tp_count), device_id_type=pl.DeviceIdType.MESH
        )

    pl.semaphore_wait(barrier, sp_count * tp_count)

    def block(m, zz, h):
        return wbuf.at[m, zz, :, cols(h, depth)]

    def half_of(m, h):
        at = pl.ds(pl.multiple_of(h * half, half), half)
        return down_in.at[at, :] if m == 2 else wsrc.at[m, at, :]

    def place_own(m):
        wbuf[m, z, :, cols(y, depth)] = half_of(m, y)[...]

    def hop(m):
        return copy(half_of(m, 1 - y), block(m, z, y), wsend_sem.at[m, 0, 4], wrecv_sem.at[m, z, y], z, 1 - y, t)

    far = (z + 2) % 4

    def line_copies(m, own):
        h = y if own else 1 - y
        src = half_of(m, y) if own else block(m, z, h)
        slot = 0 if own else 1
        dests = ((far, None), (z + 1, z < 3), (z - 1, z > 0))
        return [
            (copy(src, block(m, z, h), wsend_sem.at[m, slot, i], wrecv_sem.at[m, z, h], dest, y, t), cond)
            for i, (dest, cond) in enumerate(dests)
        ]

    def each(copies, act):
        for one, cond in copies:
            if cond is None:
                act(one)
            else:
                pl.when(cond)(functools.partial(act, one))

    def start(one):
        one.start()

    def send_own(m):
        each(line_copies(m, True), start)

    def send_other(m):
        wait_recv(block(m, z, 1 - y), wsend_sem.at[m, 0, 4], wrecv_sem.at[m, z, 1 - y])
        each(line_copies(m, False), start)

    inner = (z > 0) & (z < 3)

    def relay(m, h):
        return copy(
            block(m, far, h), block(m, far, h), wsend_sem.at[m, h, 3], wrecv_sem.at[m, far, h], 3 * (z - 1), y, t
        )

    def pass_line(m, h):
        @pl.when(inner)
        def _():
            wait_recv(block(m, far, h), wsend_sem.at[m, h, 3], wrecv_sem.at[m, far, h])
            relay(m, h).start()

    def tp_copies(src, buf, send, recv):
        return (
            copy(src, buf.at[t], send.at[0], recv.at[t], z, y, t_core),
            copy(src, buf.at[t], send.at[1], recv.at[t], z, y, t_chip),
        )

    def tp_relay(buf, send, recv):
        return copy(buf.at[t_chip], buf.at[t_chip], send.at[2], recv.at[t_chip], z, y, t_core)

    def tp_pass_on(buf, send, recv):
        wait_recv(buf.at[t_chip], send.at[2], recv.at[t_chip])
        tp_relay(buf, send, recv).start()

    def tp_arrive(buf, send, recv):
        wait_recv(buf.at[t_core], send.at[0], recv.at[t_core])
        wait_recv(buf.at[t_diag], send.at[0], recv.at[t_diag])

    hop(0).start()
    send_own(0)
    own_out = pltpu.make_async_copy(osrc, obuf.at[t], orecv_sem.at[t])
    own_out.start()
    for one in tp_copies(osrc, obuf, osend_sem, orecv_sem):
        one.start()
    wsrc[1] = jnp.transpose(value_in[...])
    for m in range(3):
        place_own(m)

    scale = DK ** (-0.5)
    key_lanes = q.shape[1]
    val_lanes = v.shape[1]
    lane_head = lax.broadcasted_iota(jnp.int32, (BLOCK, key_lanes), 1) // DK
    heads = key_lanes // DK
    low = lax.broadcasted_iota(jnp.int32, (BLOCK, BLOCK), 0) >= lax.broadcasted_iota(jnp.int32, (BLOCK, BLOCK), 1)
    low_ones = low.astype(jnp.float32)
    same_head = (
        lax.broadcasted_iota(jnp.int32, (val_lanes, key_lanes), 0) // DV
        == lax.broadcasted_iota(jnp.int32, (val_lanes, key_lanes), 1) // DK
    )
    state[...] = jnp.zeros_like(state)
    before[...] = jnp.zeros_like(before)

    def attend_block(i):
        at = pl.ds(pl.multiple_of(i * BLOCK, BLOCK), BLOCK)
        rate = logr[at, :]
        cum = jnp.dot(low_ones, rate, precision=highest, preferred_element_type=jnp.float32)
        total = cum[BLOCK - 1 :, :]
        ahead = before[0:1, :]
        q_decayed = q[at, :].astype(jnp.float32) * scale * jnp.exp(cum)
        qs[at, :] = q[at, :].astype(jnp.float32) * scale * jnp.exp(cum + ahead)
        keys = k[at, :].astype(jnp.float32)
        grown = keys * jnp.exp(-cum)
        ending = keys * jnp.exp(total - cum)
        values = v[at, :].astype(jnp.float32)
        inside = []
        for h in range(heads):
            mine = lane_head == h
            scores = nt_dot(jnp.where(mine, q_decayed, 0.0), jnp.where(mine, grown, 0.0), highest)
            scores = jnp.where(low, scores, 0.0)
            inside.append(
                jnp.dot(
                    scores, values[:, h * DV : (h + 1) * DV], precision=highest, preferred_element_type=jnp.float32
                )
            )
        old = state[...]
        mech[at, :] = jnp.concatenate(inside, axis=1) + nt_dot(q_decayed, old, highest)
        step = lax.dot_general(
            values, ending, (((0,), (0,)), ((), ())), precision=highest, preferred_element_type=jnp.float32
        )
        state[...] = old * jnp.exp(total) + jnp.where(same_head, step, 0.0)
        before[...] = jnp.broadcast_to(ahead + total, before.shape)

    blocks = tok_rows // BLOCK
    pl.loop(0, blocks)(attend_block)

    whole = state[0:DV, :]
    for h in range(1, heads):
        whole = whole + state[h * DV : (h + 1) * DV, :]
    packed[0:DV, :] = whole
    packed[DV:, :] = jnp.exp(before[...])
    pairs = sp_count // 2

    def pair_copy():
        return copy(packed, got.at[0], ssend_sem.at[0], srecv_sem.at[0], z, 1 - y, t)

    def state_copy(d):
        return copy(joined, got.at[d], ssend_sem.at[d], srecv_sem.at[d], z + d, y, t)

    pair_copy().start()
    hop(1).start()
    hop(2).start()
    wait_recv(got.at[0], ssend_sem.at[0], srecv_sem.at[0])
    early = jnp.where(first, packed[...], got[0])
    late = jnp.where(first, got[0], packed[...])
    joined[0:DV, :] = early[0:DV, :] * late[DV : DV + 1, :] + late[0:DV, :]
    joined[DV:, :] = early[DV:, :] * late[DV:, :]
    for d in range(1, pairs):
        pl.when(z + d < pairs)(functools.partial(start, state_copy(d)))
    send_other(0)
    send_own(1)
    arrived[...] = jnp.zeros_like(arrived)
    before[...] = jnp.ones_like(before)
    for d in range(1, pairs):
        @pl.when(z >= d)
        def _(d=d):
            wait_recv(got.at[d], ssend_sem.at[d], srecv_sem.at[d])
            arrived[...] += before[0:1, :] * got[d, 0:DV, :]
            before[...] = before[...] * got[d, DV:, :]

    @pl.when(y == 1)
    def _():
        arrived[...] = arrived[...] * got[0, DV : DV + 1, :] + got[0, 0:DV, :]

    lane_wide = lax.broadcasted_iota(jnp.int32, (share, key_lanes), 1) // DK
    lane_state = lax.broadcasted_iota(jnp.int32, (DV, key_lanes), 1) // DK

    @pl.loop(0, tok_rows // share)
    def _(i):
        at = pl.ds(pl.multiple_of(i * share, share), share)
        for h in range(heads):
            part = pl.ds(h * DV, DV)
            extra = nt_dot(
                jnp.where(lane_wide == h, qs[at, :], 0.0), jnp.where(lane_state == h, arrived[...], 0.0), highest
            )
            o = mech[at, part] + extra
            o = o * lax.rsqrt(jnp.mean(o * o, axis=-1, keepdims=True) + eps) * hgain[...]
            gate = gates[at, part].astype(jnp.float32)
            mixbuf[t, at, part] = (o * (gate * jax.nn.sigmoid(gate))).astype(jnp.bfloat16)

    for one in tp_copies(mixbuf.at[t], mixbuf, msend_sem, mrecv_sem):
        one.start()
    tp_pass_on(obuf, osend_sem, orecv_sem)
    send_other(1)
    tp_pass_on(mixbuf, msend_sem, mrecv_sem)
    own_out.wait()
    tp_arrive(obuf, osend_sem, orecv_sem)
    pass_line(0, y)
    tp_arrive(mixbuf, msend_sem, mrecv_sem)

    def tile_at(yy, tile):
        return pl.ds(pl.multiple_of(EDGE + yy * tok_rows + tile * share, EDGE), share)

    def tile_copy(i, tile):
        ref = rows.at[tile_at(y, tile), :]
        return copy(ref, ref, tsend_sem.at[i], trecv_sem.at[tile], z, 1 - y, t)

    @pl.loop(0, tp_count)
    def _(i):
        tile = (2 * c + i) % tp_count
        at = pl.ds(pl.multiple_of(tile * share, share), share)
        total = res[at, :].astype(jnp.float32)
        for part in range(tp_count):
            total = total + jnp.dot(mixbuf[part, at, :], obuf[part], preferred_element_type=jnp.float32)
        scaled = total * lax.rsqrt(jnp.mean(total * total, axis=-1, keepdims=True) + eps)
        rows[tile_at(y, tile), :] = (scaled * fgain[...]).astype(jnp.bfloat16)

        @pl.when(tile == t)
        def _():
            resid[...] = total

        @pl.when(i < 2)
        def _():
            tile_copy(i, tile).start()

    last = rows.at[pl.ds(EDGE + 2 * tok_rows - EDGE, EDGE), :]
    head = rows.at[pl.ds(0, EDGE), :]

    def edge_copy(yy):
        return copy(last, head, tsend_sem.at[4 + yy], trecv_sem.at[tp_count], z + 1, yy, t)

    @pl.when((y == 1) & (z < 3))
    def _():
        edge_copy(0).start()
        edge_copy(1).start()

    @pl.when(z == 0)
    def _():
        rows[0:EDGE, :] = jnp.zeros((EDGE, rows.shape[1]), rows.dtype)

    pass_line(0, 1 - y)
    send_own(2)
    send_other(2)

    def pass_copy(i):
        ref = rows.at[tile_at(1 - y, 2 * c + i), :]
        return copy(ref, ref, tsend_sem.at[2 + i], trecv_sem.at[2 * c + i], z, y, t_core)

    towards = jnp.where(z < 2, 1, 3)

    def source(step):
        return (z + step * towards) % 4

    def weights_here(m, step):
        zk = source(step)
        if step > 0:
            @pl.when(jnp.logical_not(inner & (zk == far)))
            def _():
                for h in range(2):
                    wait_recv(block(m, zk, h), wsend_sem.at[m, h, 3], wrecv_sem.at[m, zk, h])

    def project(m, step, first_row, size, tiles):
        zk = source(step)

        def tile(i):
            at = pl.ds(pl.multiple_of(first_row + i * size, EDGE), size)
            part = nt_dot(rows[at, cols(zk, wide)], wbuf[m, zk])
            if step == 0:
                acc[m, at, :] = part
            else:
                acc[m, at, :] += part

        if tiles == 1:
            tile(0)
        else:
            pl.loop(0, tiles)(tile)

    tall = tok_rows // 2
    for m in range(2):
        for step in range(4):
            weights_here(m, step)
            project(m, step, EDGE + y * tok_rows, tall, 2)
        if m == 0:
            for i in range(2):
                ref = rows.at[tile_at(1 - y, 2 * c + i), :]
                wait_recv(ref, tsend_sem.at[2 + i], trecv_sem.at[2 * c + i])
                pass_copy(i).start()
            pass_line(1, y)
            pass_line(1, 1 - y)
    for i in range(2):
        ref = rows.at[tile_at(1 - y, 2 * (1 - c) + i), :]
        wait_recv(ref, tsend_sem.at[2 + i], trecv_sem.at[2 * (1 - c) + i])

    @pl.when(z > 0)
    def _():
        wait_recv(head, tsend_sem.at[4], trecv_sem.at[tp_count])

    for m in range(2):
        for step in range(4):
            project(m, step, EDGE + (1 - y) * tok_rows, tall, 2)
            project(m, step, 0, EDGE, 1)

    @pl.loop(0, 2 * tok_rows // share)
    def _(i):
        at = pl.ds(pl.multiple_of(i * share, EDGE), share + EDGE)

        def mix(m):
            up = acc[m, at, :].astype(jnp.bfloat16).astype(jnp.float32)
            total = jnp.zeros_like(up)
            for j in range(CONV):
                back = CONV - 1 - j
                moved = up if back == 0 else pltpu.roll(up, back, 0)
                total = total + taps[m * CONV + j : m * CONV + j + 1, :] * moved
            return total[EDGE:, :]

        gate = mix(0)
        to = pl.ds(pl.multiple_of(i * share, share), share)
        hid[to, :] = (gate * jax.nn.sigmoid(gate) * mix(1)).astype(jnp.bfloat16)

    pass_line(2, y)
    pass_line(2, 1 - y)

    count = 8

    def down(b):
        step, h = b // 2, b % 2
        if h == 0:
            weights_here(2, step)
        weight = wbuf[2, source(step), :, h * depth : (h + 1) * depth]

        @pl.loop(0, tp_count)
        def _(j):
            give = pl.ds(pl.multiple_of((2 * j + 1 - c) * share, share), share)
            keep = pl.ds(pl.multiple_of((2 * j + c) * share, share), share)
            csend[b, j] = jnp.dot(hid[give, :], weight, preferred_element_type=jnp.float32).astype(jnp.bfloat16)
            ckeep[b % 2, j] = jnp.dot(hid[keep, :], weight, preferred_element_type=jnp.float32)

        c_copy(b).start()

    def c_copy(b):
        return copy(csend.at[b], crecv.at[b], csend_sem.at[b], crecv_sem.at[b], z, y, t_core)

    def second(b):
        to = (z, 1 - y, t) if b % 2 == 0 else (z, y, t_chip)
        return copy(ysend.at[b], yrecv.at[b], ysend_sem.at[b], yrecv_sem.at[b], *to)

    def third(b):
        to = (z, y, t_chip) if b % 2 == 0 else (z, 1 - y, t)
        return copy(xsend.at[b], xrecv.at[b], xsend_sem.at[b], xrecv_sem.at[b], *to)

    def over_c(b):
        c_copy(b).wait()
        even = b % 2 == 0
        for i in range(2):
            j = (1 - y) * 2 + i if even else i * 2 + 1 - x
            ysend[b, i] = (ckeep[b % 2, j] + crecv[b, j].astype(jnp.float32)).astype(jnp.bfloat16)
        second(b).start()
        for i in range(2):
            j = y * 2 + i if even else i * 2 + x
            ykeep[b % 2, i] = ckeep[b % 2, j] + crecv[b, j].astype(jnp.float32)

    def over_second(b):
        second(b).wait()
        keep = x if b % 2 == 0 else y
        xsend[b] = (ykeep[b % 2, 1 - keep] + yrecv[b, 1 - keep].astype(jnp.float32)).astype(jnp.bfloat16)
        third(b).start()
        xkeep[b % 2] = ykeep[b % 2, keep] + yrecv[b, keep].astype(jnp.float32)

    def over_third(b):
        third(b).wait()
        at = pl.ds(pl.multiple_of(source(b // 2) * wide + b % 2 * depth, depth), depth)
        total = resid[:, at] + (xkeep[b % 2] + xrecv[b].astype(jnp.float32))
        out[:, at] = total.astype(out.dtype)

    for b in range(count + 5):
        if 0 <= b - 5:
            over_third(b - 5)
        if 0 <= b - 3 < count:
            over_second(b - 3)
        if 0 <= b - 1 < count:
            over_c(b - 1)
        if b < count:
            down(b)

    def finish(one):
        one.wait_send()

    for m in range(3):
        finish(hop(m))
        each(line_copies(m, True), finish)
        each(line_copies(m, False), finish)

        @pl.when(inner)
        def _(m=m):
            for h in range(2):
                finish(relay(m, h))
    for src, buf, send, recv in (
        (osrc, obuf, osend_sem, orecv_sem),
        (mixbuf.at[t], mixbuf, msend_sem, mrecv_sem),
    ):
        for one in tp_copies(src, buf, send, recv):
            finish(one)
        finish(tp_relay(buf, send, recv))
    finish(pair_copy())
    for d in range(1, pairs):
        pl.when(z + d < pairs)(functools.partial(finish, state_copy(d)))
    for i in range(2):
        finish(tile_copy(i, 2 * c + i))
        finish(pass_copy(i))

    @pl.when((y == 1) & (z < 3))
    def _():
        finish(edge_copy(0))
        finish(edge_copy(1))


def fused_layer(
    residual_input_stream,
    projected_queries,
    projected_keys,
    projected_values,
    emitted_switch_entries,
    retention_preactivations,
    additional_fading_amount,
    head_norm_gain,
    attention_output_weight,
    feedforward_norm_gain,
    gate_up_matrix,
    value_up_matrix,
    gate_filter_taps,
    value_filter_taps,
    down_projection_weight,
):
    tok_rows, width = residual_input_stream.shape
    keys, vals = projected_queries.shape[1], projected_values.shape[1]
    depth, units = gate_up_matrix.shape
    half, tp = units // 2, lax.axis_size("tp")
    share = tok_rows // tp
    rates = (
        jax.nn.log_sigmoid(retention_preactivations.astype(jnp.float32)) / retention_sharpness
        + additional_fading_amount[:, None]
    )
    bf16, f32, dma = jnp.bfloat16, jnp.float32, pltpu.SemaphoreType.DMA
    hbm, vmem = pl.BlockSpec(memory_space=pl.ANY), pl.BlockSpec(memory_space=pltpu.VMEM)
    scratch = [
        pltpu.VMEM((2, units, depth), bf16),
        pltpu.VMEM((8, half), f32),
        pltpu.VMEM((3, 4, half, 2 * depth), bf16),
        pltpu.VMEM((tp, vals, width), bf16),
        pltpu.VMEM((tp, tok_rows, vals), bf16),
        pltpu.VMEM((EDGE + 2 * tok_rows, width), bf16),
        pltpu.VMEM((2, EDGE + 2 * tok_rows, half), f32),
        pltpu.VMEM((2 * tok_rows, half), bf16),
        pltpu.VMEM((tok_rows, vals), f32),
        pltpu.VMEM((tok_rows, keys), f32),
        pltpu.VMEM((vals, keys), f32),
        pltpu.VMEM((8, keys), f32),
        pltpu.VMEM((DV + 8, keys), f32),
        pltpu.VMEM((DV + 8, keys), f32),
        pltpu.VMEM((4, DV + 8, keys), f32),
        pltpu.VMEM((DV, keys), f32),
        pltpu.VMEM((share, width), f32),
        pltpu.VMEM((8, 4, share, depth), bf16),
        pltpu.VMEM((8, 4, share, depth), bf16),
        pltpu.VMEM((2, 4, share, depth), f32),
        pltpu.VMEM((8, 2, share, depth), bf16),
        pltpu.VMEM((8, 2, share, depth), bf16),
        pltpu.VMEM((2, 2, share, depth), f32),
        pltpu.VMEM((8, share, depth), bf16),
        pltpu.VMEM((8, share, depth), bf16),
        pltpu.VMEM((2, share, depth), f32),
        dma((3, 4, 2)), dma((3, 2, 5)), dma((tp,)), dma((3,)), dma((tp,)), dma((3,)), dma((4,)), dma((4,)),
        dma((tp + 1,)), dma((6,)), dma((8,)), dma((8,)), dma((8,)), dma((8,)), dma((8,)), dma((8,)),
    ]
    return pl.pallas_call(
        layer_kernel,
        name="layer",
        out_shape=jax.ShapeDtypeStruct((share, width), bf16),
        in_specs=[vmem] * 3 + [hbm] + [vmem] * 10,
        out_specs=vmem,
        scratch_shapes=scratch,
        compiler_params=pltpu.CompilerParams(
            collective_id=0, has_side_effects=True, vmem_limit_bytes=67043328
        ),
    )(
        gate_up_matrix, value_up_matrix, down_projection_weight, attention_output_weight, projected_queries, projected_keys, projected_values,
        emitted_switch_entries, rates, residual_input_stream, head_norm_gain[None], feedforward_norm_gain[None],
        gate_filter_taps, value_filter_taps,
    )


def specs(rows):
    return (
            P(rows, None),
            P(rows, "tp"),
            P(rows, "tp"),
            P(rows, "tp"),
            P(rows, "tp"),
            P(rows, "tp"),
            P(rows),
            P(),
            P("tp", None),
            P(),
            P(rows, "tp"),
            P(rows, "tp"),
            P(None, "tp"),
            P(None, "tp"),
            P("tp", rows),
    )


def solution(mesh):
    sp, tp = mesh.shape["sp"], mesh.shape["tp"]
    if sp == 8 and tp == 4:
        return jax.shard_map(
            fused_layer,
            mesh=mesh,
            in_specs=specs("sp"),
            out_specs=P(("sp", "tp"), None),
            check_vma=False,
        )
    split = Mesh(mesh.devices.reshape(sp // 2, 2, tp), ("so", "si", "tp"))
    return jax.shard_map(
        per_device, mesh=split, in_specs=specs(SP), out_specs=P(("so", "si", "tp"), None), check_vma=False
    )
```

```python
import functools

import jax
import jax.numpy as jnp
from jax import lax
from jax.experimental import pallas as pl
from jax.experimental.pallas import tpu as pltpu
from jax.sharding import Mesh, PartitionSpec as P

DK = 64
DV = 128
CONV = 3
BLOCK = 64
EDGE = 16
SP = ("so", "si")


eps = 1e-06
retention_sharpness = 16.0


def from_behind(block, axis, distance):
    devices = range(lax.axis_size(axis))
    route = [(i - distance, i) for i in devices if i - distance in devices]
    return lax.ppermute(block, axis, route)


def to_blocks(tensor, local_heads, width):
    count = tensor.shape[0] // BLOCK
    return tensor.astype(jnp.float32).reshape(count, BLOCK, local_heads, width)


def row_norm(stream, gain):
    scaled = stream * lax.rsqrt(jnp.mean(stream * stream, axis=-1, keepdims=True) + eps)
    return (scaled * gain).astype(jnp.bfloat16)


def state_before_device(dev_log, dev_state):
    heads, channels, width = dev_state.shape
    lanes = heads * channels
    decay = jnp.pad(jnp.exp(dev_log).reshape(1, lanes), ((0, 0), (0, -lanes % width)))
    decay = decay.reshape(-1, width)
    packed = jnp.concatenate([dev_state.reshape(lanes, width), decay], axis=0)
    arriving = jnp.zeros_like(dev_state)
    after = jnp.ones((heads, channels), jnp.float32)
    for distance in range(1, lax.axis_size("so") * lax.axis_size("si")):
        got = from_behind(packed, SP, distance)
        arriving = arriving + after[..., None] * got[:lanes].reshape(dev_state.shape)
        after = after * got[lanes:].reshape(-1)[:lanes].reshape(after.shape)
    return arriving


def xor_route(axis, bit):
    return [(i, i ^ bit) for i in range(lax.axis_size(axis))]


def exchange(block, axis, bit):
    return lax.ppermute(block, axis, xor_route(axis, bit))


def gather_tp(block):
    count, me = lax.axis_size("tp"), lax.axis_index("tp")
    held = block[None]
    bit = count // 2
    while bit:
        other = exchange(held, "tp", bit)
        low = (me & bit) == 0
        held = jnp.stack([jnp.where(low, held, other), jnp.where(low, other, held)])
        held = held.reshape((-1,) + block.shape)
        bit //= 2
    bits = count.bit_length() - 1
    order = [sum(((t >> b) & 1) << (bits - 1 - b) for b in range(bits)) for t in range(count)]
    return [held[o] for o in order]


def swap_halves(block):
    first = lax.axis_index("si") == 0
    half = block.shape[0] // 2
    low, high = block[:half], block[half:]
    keep, give = jnp.where(first, low, high), jnp.where(first, high, low)
    got = exchange(give, "si", 1)
    return jnp.concatenate([jnp.where(first, keep, got), jnp.where(first, got, keep)], axis=1)


def line_gather(block):
    count, me = lax.axis_size("so"), lax.axis_index("so")
    if count != 4:
        whole = lax.all_gather(block, "so", axis=0)
        return [lax.dynamic_index_in_dim(whole, (me + k) % count, 0, False) for k in range(count)]
    across = lax.ppermute(block, "so", [(i, i ^ 2) for i in range(4)])
    above = lax.ppermute(block, "so", [(1, 0), (2, 1), (3, 2)])
    below = lax.ppermute(block, "so", [(0, 1), (1, 2), (2, 3)])
    far = lax.ppermute(across, "so", [(1, 0), (2, 3)])
    return [block, jnp.where(me == 3, far, above), across, jnp.where(me == 0, far, below)]


def pair_rows(normed):
    share = normed.shape[0] // 2
    mine = lax.axis_index("tp") % 2
    part = exchange(lax.dynamic_slice_in_dim(normed, mine * share, share, 0), "si", 1)
    other = exchange(part, "tp", 1)
    first = mine == 0
    return jnp.concatenate([jnp.where(first, part, other), jnp.where(first, other, part)], axis=0)


def project(rows, lines, width):
    count, me = lax.axis_size("so"), lax.axis_index("so")
    total = 0.0
    for k, line in enumerate(lines):
        part = lax.dynamic_slice_in_dim(rows, (me + k) % count * width, width, 1)
        total = total + lax.dot_general(
            part, line, (((1,), (1,)), ((), ())), preferred_element_type=jnp.float32
        )
    return total.astype(jnp.bfloat16)


def depthwise(before, body, taps):
    padded = jnp.concatenate([before, body], axis=0)
    start = padded.shape[0] - body.shape[0] - (CONV - 1)
    result = jnp.zeros(body.shape, jnp.float32)
    for offset in range(CONV):
        result = result + taps[offset].astype(jnp.float32)[None] * padded[
            start + offset : start + offset + body.shape[0]
        ].astype(jnp.float32)
    return result


def my_half(taps):
    half = taps.shape[1] // 2
    return jnp.where(lax.axis_index("si") == 0, taps[:, :half], taps[:, half:])


def halve(held, axis, bit):
    mine = (lax.axis_index(axis) // bit) % 2
    keep = lax.dynamic_index_in_dim(held, mine, 1, False)
    give = lax.dynamic_index_in_dim(held, 1 - mine, 1, False)
    got = exchange(give.astype(jnp.bfloat16), axis, bit)
    return keep.astype(jnp.float32) + got.astype(jnp.float32)


def scatter_sum(own, other):
    count = lax.axis_size("tp")
    share = own.shape[0] // count
    held = jnp.concatenate([own, other], axis=0)
    held = halve(held.reshape(count, 2, share, -1), "tp", 1)
    held = held.reshape(2, count // 2, share, -1)
    got = exchange(held[1].astype(jnp.bfloat16), "si", 1)
    held = held[0] + got.astype(jnp.float32)
    bit = 2
    while bit < count:
        held = halve(held.reshape((-1, 2) + held.shape[1:]), "tp", bit)
        bit *= 2
    return held[0]


def per_device(
    residual_input_stream,
    projected_queries,
    projected_keys,
    projected_values,
    emitted_switch_entries,
    retention_preactivations,
    additional_fading_amount,
    head_norm_gain,
    attention_output_weight,
    feedforward_norm_gain,
    gate_up_matrix,
    value_up_matrix,
    gate_filter_taps,
    value_filter_taps,
    down_projection_weight,
):
    largest_exponent = lax.Precision.HIGHEST
    tok_rows = residual_input_stream.shape[0]
    local_heads = projected_queries.shape[1] // DK
    gate_lines = line_gather(swap_halves(gate_up_matrix.T))
    value_lines = line_gather(swap_halves(value_up_matrix.T))
    down_lines = line_gather(swap_halves(down_projection_weight))
    out_full = jnp.concatenate(gather_tp(attention_output_weight), axis=0)
    retention_logarithm = (
        jax.nn.log_sigmoid(retention_preactivations.astype(jnp.float32)) / retention_sharpness
        + additional_fading_amount[:, None]
    )
    scaled_q = to_blocks(projected_queries, local_heads, DK) * DK ** (-0.5)
    key_heads = to_blocks(projected_keys, local_heads, DK)
    value_heads = to_blocks(projected_values, local_heads, DV)
    rate_cum = jnp.cumsum(to_blocks(retention_logarithm, local_heads, DK), axis=1)
    block_total = rate_cum[:, -1]
    before_block = jnp.cumsum(block_total, axis=0) - block_total
    q_decayed = scaled_q * jnp.exp(rate_cum)
    k_growth = key_heads * jnp.exp(-rate_cum)
    fading_through_finish = key_heads * jnp.exp(block_total[:, None] - rate_cum)
    lower = jnp.tril(jnp.ones((BLOCK, BLOCK), bool))
    scores = jnp.einsum("nihk,njhk->nhij", q_decayed, k_growth, precision=largest_exponent)
    scores = jnp.where(lower[None, None], scores, 0.0)
    within = jnp.einsum("nhij,njhv->nihv", scores, value_heads, precision=largest_exponent)
    increments = jnp.einsum(
        "nchk,nchv->nhkv", fading_through_finish, value_heads, precision=largest_exponent
    )

    count = block_total.shape[0]
    ends = before_block + block_total
    reached = jnp.concatenate([before_block, ends[-1:]], axis=0)
    earlier_block = jnp.arange(count)[None, :] < jnp.arange(count + 1)[:, None]
    fade = jnp.where(
        earlier_block[..., None, None],
        jnp.exp(jnp.minimum(reached[:, None] - ends[None], 0.0)),
        0.0,
    )
    states = jnp.sum(fade[..., None] * increments[None], axis=1)
    state_before, dev_state = states[:-1], states[-1]
    earlier = jnp.einsum("nchk,nhkv->nchv", q_decayed, state_before, precision=largest_exponent)
    query_shard = scaled_q * jnp.exp(rate_cum + before_block[:, None])
    dev_log = jnp.sum(block_total, axis=0)

    arriving_state = state_before_device(dev_log, dev_state)
    earlier_memory_share = jnp.einsum(
        "osyq,yqi->osyi", query_shard, arriving_state, precision=largest_exponent
    )
    mech_out = (within + earlier + earlier_memory_share).reshape(tok_rows, local_heads, DV)
    mech_out = (
        mech_out
        * lax.rsqrt(jnp.mean(mech_out * mech_out, axis=-1, keepdims=True) + eps)
        * head_norm_gain
    )
    mixed = (
        mech_out.reshape(tok_rows, local_heads * DV)
        * jax.nn.silu(emitted_switch_entries.astype(jnp.float32))
    ).astype(jnp.bfloat16)
    tp_count, tp_index = (lax.axis_size("tp"), lax.axis_index("tp"))
    share = tok_rows // tp_count
    mixed_all = jnp.concatenate(gather_tp(mixed), axis=1)
    attended = jnp.dot(mixed_all, out_full, preferred_element_type=jnp.float32)
    resid = residual_input_stream.astype(jnp.float32) + attended
    normed = row_norm(resid, feedforward_norm_gain)
    resid_own = lax.dynamic_slice_in_dim(resid, tp_index * share, share, 0)
    edge = normed[tok_rows - EDGE :]
    so_count, so_index = lax.axis_size("so"), lax.axis_index("so")
    first = lax.axis_index("si") == 0
    tail = jnp.where(first, from_behind(edge, SP, 1), from_behind(edge, "so", 1))
    width = 2 * gate_up_matrix.shape[0]
    other = pair_rows(normed)
    mine = jnp.concatenate([tail, normed], axis=0)
    gate_own = project(mine, gate_lines, width)
    value_own = project(mine, value_lines, width)
    gate_other = project(other, gate_lines, width)
    value_other = project(other, value_lines, width)

    def mix(up_own, up_other, taps):
        taps = my_half(taps)
        up_tail, up_own = up_own[:EDGE], up_own[EDGE:]
        own_end, other_end = up_own[tok_rows - EDGE :], up_other[tok_rows - EDGE :]
        own = depthwise(jnp.where(first, up_tail, other_end), up_own, taps)
        far = depthwise(jnp.where(first, own_end, up_tail), up_other, taps)
        return own, far

    gates = mix(gate_own, gate_other, gate_filter_taps)
    values = mix(value_own, value_other, value_filter_taps)
    hidden = [(jax.nn.silu(g) * v).astype(jnp.bfloat16) for g, v in zip(gates, values)]
    feed = jnp.zeros((share, resid.shape[1]), jnp.float32)
    for k, line in enumerate(down_lines):
        part = scatter_sum(*[jnp.dot(h, line, preferred_element_type=jnp.float32) for h in hidden])
        feed = lax.dynamic_update_slice_in_dim(feed, part, (so_index + k) % so_count * width, 1)
    return (resid_own + feed).astype(jnp.bfloat16)


def nt_dot(a, b, precision=None):
    return lax.dot_general(
        a, b, (((1,), (1,)), ((), ())), precision=precision, preferred_element_type=jnp.float32
    )


def layer_kernel(
    gate_in, value_in, down_in, osrc, q, k, v, gates, retention, fading, res, hgain, fgain, gate_taps, value_taps,
    out,
    wsrc, taps, wbuf, obuf, mixbuf, rows, acc, hid, mech, qs, state, before, packed, joined, edge, got, arrived, resid,
    csend, crecv, ckeep, ysend, yrecv, ykeep, xsend, xrecv, xkeep,
    wrecv_sem, wsend_sem, orecv_sem, osend_sem, mrecv_sem, msend_sem, srecv_sem, ssend_sem,
    trecv_sem, tsend_sem, crecv_sem, csend_sem, yrecv_sem, ysend_sem, xrecv_sem, xsend_sem,
):
    highest = lax.Precision.HIGHEST
    s, t = lax.axis_index("sp"), lax.axis_index("tp")
    z, y, x, c = s // 2, s % 2, t // 2, t % 2
    sp_count, tp_count = lax.axis_size("sp"), lax.axis_size("tp")
    tok_rows, (units, depth) = q.shape[0], down_in.shape
    half = units // 2
    share = out.shape[0]
    wide = 2 * depth

    def copy(src, dst, send, recv, zz, yy, tt):
        return pltpu.make_async_remote_copy(
            src_ref=src, dst_ref=dst, send_sem=send, recv_sem=recv,
            device_id=(zz * 2 + yy, tt), device_id_type=pl.DeviceIdType.MESH,
        )

    def wait_recv(ref, send, recv):
        copy(ref, ref, send, recv, z, y, t).wait_recv()

    def wait_send(ref, send, recv):
        copy(ref, ref, send, recv, z, y, t).wait_send()

    def cols(index, width):
        return pl.ds(pl.multiple_of(index * width, width), width)

    t_core, t_chip, t_diag = x * 2 + 1 - c, (1 - x) * 2 + c, (1 - x) * 2 + 1 - c

    wsrc[0] = jnp.transpose(gate_in[...])
    first = y == 0
    for m, given in enumerate((gate_taps, value_taps)):
        both = given[...].astype(jnp.float32)
        taps[m * CONV : (m + 1) * CONV, :] = jnp.where(first, both[:, :half], both[:, half:])

    barrier = pltpu.get_barrier_semaphore()

    @pl.loop(0, sp_count * tp_count)
    def _(i):
        pl.semaphore_signal(
            barrier, inc=1, device_id=(i // tp_count, i % tp_count), device_id_type=pl.DeviceIdType.MESH
        )

    pl.semaphore_wait(barrier, sp_count * tp_count)

    def block(m, zz, h):
        return wbuf.at[m, zz, :, cols(h, depth)]

    def half_of(m, h):
        at = pl.ds(pl.multiple_of(h * half, half), half)
        return down_in.at[at, :] if m == 2 else wsrc.at[m, at, :]

    def place_own(m):
        wbuf[m, z, :, cols(y, depth)] = half_of(m, y)[...]

    def hop(m):
        return copy(half_of(m, 1 - y), block(m, z, y), wsend_sem.at[m, 0, 4], wrecv_sem.at[m, z, y], z, 1 - y, t)

    far = (z + 2) % 4

    def line_copies(m, slot):
        h = slot if m == 2 else (y if slot == 0 else 1 - y)
        src = half_of(m, y) if m < 2 and slot == 0 else block(m, z, h)
        dests = ((far, None), (z + 1, z < 3), (z - 1, z > 0))
        return [
            (copy(src, block(m, z, h), wsend_sem.at[m, slot, i], wrecv_sem.at[m, z, h], dest, y, t), cond)
            for i, (dest, cond) in enumerate(dests)
        ]

    def each(copies, act):
        for one, cond in copies:
            if cond is None:
                act(one)
            else:
                pl.when(cond)(functools.partial(act, one))

    def start(one):
        one.start()

    inner = (z > 0) & (z < 3)

    def near_copies(m, slot):
        each(line_copies(m, slot)[1:], start)

    def outer_far(m, slot):
        pl.when(jnp.logical_not(inner))(functools.partial(start, line_copies(m, slot)[0][0]))

    def relay(m, h, origin):
        zz, index = (far, 3) if origin == "far" else (3 - z, 0)
        return copy(
            block(m, zz, h), block(m, zz, h), wsend_sem.at[m, h, index], wrecv_sem.at[m, zz, h], 3 * (z - 1), y, t
        )

    def pass_line(m, h, origin):
        @pl.when(inner)
        def _():
            zz, index = (far, 3) if origin == "far" else (3 - z, 0)
            wait_recv(block(m, zz, h), wsend_sem.at[m, h, index], wrecv_sem.at[m, zz, h])
            relay(m, h, origin).start()

    def tp_copies(src, buf, send, recv):
        return (
            copy(src, buf.at[t], send.at[0], recv.at[t], z, y, t_core),
            copy(src, buf.at[t], send.at[1], recv.at[t], z, y, t_chip),
        )

    def tp_relay(buf, send, recv):
        return copy(buf.at[t_chip], buf.at[t_chip], send.at[2], recv.at[t_chip], z, y, t_core)

    def tp_pass_on(buf, send, recv):
        wait_recv(buf.at[t_chip], send.at[2], recv.at[t_chip])
        tp_relay(buf, send, recv).start()

    def tp_arrive(buf, send, recv):
        wait_recv(buf.at[t_core], send.at[0], recv.at[t_core])
        wait_recv(buf.at[t_diag], send.at[0], recv.at[t_diag])

    hop(0).start()
    near_copies(0, 0)
    own_out = pltpu.make_async_copy(osrc, obuf.at[t], orecv_sem.at[t])
    own_out.start()
    for one in tp_copies(osrc, obuf, osend_sem, orecv_sem):
        one.start()
    wsrc[1] = jnp.transpose(value_in[...])
    hop(1).start()
    for m in range(3):
        place_own(m)

    scale = DK ** (-0.5)
    key_lanes = q.shape[1]
    val_lanes = v.shape[1]
    lane_head = lax.broadcasted_iota(jnp.int32, (BLOCK, key_lanes), 1) // DK
    heads = key_lanes // DK
    low = lax.broadcasted_iota(jnp.int32, (BLOCK, BLOCK), 0) >= lax.broadcasted_iota(jnp.int32, (BLOCK, BLOCK), 1)
    low_ones = low.astype(jnp.float32)
    same_head = (
        lax.broadcasted_iota(jnp.int32, (val_lanes, key_lanes), 0) // DV
        == lax.broadcasted_iota(jnp.int32, (val_lanes, key_lanes), 1) // DK
    )
    state[...] = jnp.zeros_like(state)
    before[...] = jnp.zeros_like(before)

    def attend_block(i):
        at = pl.ds(pl.multiple_of(i * BLOCK, BLOCK), BLOCK)
        gate = retention[at, :].astype(jnp.float32)
        rate = (jnp.minimum(gate, 0.0) - jnp.log1p(jnp.exp(-jnp.abs(gate)))) / retention_sharpness
        faded = jnp.sum(jnp.where(low, fading[pl.ds(i, 1), :], 0.0), axis=1, keepdims=True)
        cum = jnp.dot(low_ones, rate, precision=highest, preferred_element_type=jnp.float32) + faded
        total = cum[BLOCK - 1 :, :]
        ahead = before[0:1, :]
        q_decayed = q[at, :].astype(jnp.float32) * scale * jnp.exp(cum)
        qs[at, :] = q[at, :].astype(jnp.float32) * scale * jnp.exp(cum + ahead)
        keys = k[at, :].astype(jnp.float32)
        grown = keys * jnp.exp(-cum)
        ending = keys * jnp.exp(total - cum)
        values = v[at, :].astype(jnp.float32)
        inside = []
        for h in range(heads):
            mine = lane_head == h
            scores = nt_dot(jnp.where(mine, q_decayed, 0.0), jnp.where(mine, grown, 0.0), highest)
            scores = jnp.where(low, scores, 0.0)
            inside.append(
                jnp.dot(
                    scores, values[:, h * DV : (h + 1) * DV], precision=highest, preferred_element_type=jnp.float32
                )
            )
        old = state[...]
        mech[at, :] = jnp.concatenate(inside, axis=1) + nt_dot(q_decayed, old, highest)
        step = lax.dot_general(
            values, ending, (((0,), (0,)), ((), ())), precision=highest, preferred_element_type=jnp.float32
        )
        state[...] = old * jnp.exp(total) + jnp.where(same_head, step, 0.0)
        before[...] = jnp.broadcast_to(ahead + total, before.shape)

    blocks = tok_rows // BLOCK
    early_blocks = 2 * blocks // 3
    pl.loop(0, early_blocks)(attend_block)
    wait_recv(block(0, z, 1 - y), wsend_sem.at[0, 0, 4], wrecv_sem.at[0, z, 1 - y])
    near_copies(0, 1)
    pass_line(0, y, "near")
    pl.loop(early_blocks, blocks)(attend_block)

    whole = state[0:DV, :]
    for h in range(1, heads):
        whole = whole + state[h * DV : (h + 1) * DV, :]
    packed[0:DV, :] = whole
    packed[DV:, :] = jnp.exp(before[...])
    pairs = sp_count // 2

    def pair_copy():
        return copy(packed, got.at[0], ssend_sem.at[0], srecv_sem.at[0], z, 1 - y, t)

    def state_copy(d):
        return copy(joined, got.at[d], ssend_sem.at[d], srecv_sem.at[d], z + d, y, t)

    pair_copy().start()
    hop(2).start()
    wait_recv(got.at[0], ssend_sem.at[0], srecv_sem.at[0])
    early = jnp.where(first, packed[...], got[0])
    late = jnp.where(first, got[0], packed[...])
    joined[0:DV, :] = early[0:DV, :] * late[DV : DV + 1, :] + late[0:DV, :]
    joined[DV:, :] = early[DV:, :] * late[DV:, :]
    for d in range(1, pairs):
        pl.when(z + d < pairs)(functools.partial(start, state_copy(d)))
    pass_line(0, 1 - y, "near")
    near_copies(1, 0)
    arrived[...] = jnp.zeros_like(arrived)
    before[...] = jnp.ones_like(before)
    for d in range(1, pairs):
        @pl.when(z >= d)
        def _(d=d):
            wait_recv(got.at[d], ssend_sem.at[d], srecv_sem.at[d])
            arrived[...] += before[0:1, :] * got[d, 0:DV, :]
            before[...] = before[...] * got[d, DV:, :]

    @pl.when(y == 1)
    def _():
        arrived[...] = arrived[...] * got[0, DV : DV + 1, :] + got[0, 0:DV, :]

    lane_wide = lax.broadcasted_iota(jnp.int32, (share, key_lanes), 1) // DK
    lane_state = lax.broadcasted_iota(jnp.int32, (DV, key_lanes), 1) // DK

    @pl.loop(0, tok_rows // share)
    def _(i):
        at = pl.ds(pl.multiple_of(i * share, share), share)
        for h in range(heads):
            part = pl.ds(h * DV, DV)
            extra = nt_dot(
                jnp.where(lane_wide == h, qs[at, :], 0.0), jnp.where(lane_state == h, arrived[...], 0.0), highest
            )
            o = mech[at, part] + extra
            o = o * lax.rsqrt(jnp.mean(o * o, axis=-1, keepdims=True) + eps) * hgain[...]
            gate = gates[at, part].astype(jnp.float32)
            mixbuf[t, at, part] = (o * (gate * jax.nn.sigmoid(gate))).astype(jnp.bfloat16)

    for one in tp_copies(mixbuf.at[t], mixbuf, msend_sem, mrecv_sem):
        one.start()
    outer_far(0, 0)
    outer_far(0, 1)
    tp_pass_on(obuf, osend_sem, orecv_sem)
    tp_pass_on(mixbuf, msend_sem, mrecv_sem)
    own_out.wait()
    tp_arrive(obuf, osend_sem, orecv_sem)
    tp_arrive(mixbuf, msend_sem, mrecv_sem)

    def tile_at(yy, tile):
        return pl.ds(pl.multiple_of(EDGE + yy * tok_rows + tile * share, EDGE), share)

    def tile_copy(i, tile):
        ref = rows.at[tile_at(y, tile), :]
        return copy(ref, ref, tsend_sem.at[i], trecv_sem.at[tile], z, 1 - y, t)

    def stream(at):
        total = res[at, :].astype(jnp.float32)
        for part in range(tp_count):
            total = total + jnp.dot(mixbuf[part, at, :], obuf[part], preferred_element_type=jnp.float32)
        scaled = total * lax.rsqrt(jnp.mean(total * total, axis=-1, keepdims=True) + eps)
        return total, (scaled * fgain[...]).astype(jnp.bfloat16)

    head = rows.at[pl.ds(0, EDGE), :]

    def edge_copy(yy):
        return copy(edge, head, tsend_sem.at[4 + yy], trecv_sem.at[tp_count], z + 1, yy, t)

    @pl.when((y == 1) & (z < 3))
    def _():
        edge[...] = stream(pl.ds(tok_rows - EDGE, EDGE))[1]
        edge_copy(0).start()
        edge_copy(1).start()

    @pl.when(z == 0)
    def _():
        rows[0:EDGE, :] = jnp.zeros((EDGE, rows.shape[1]), rows.dtype)

    pass_line(1, y, "near")
    outer_far(1, 0)

    @pl.loop(0, tp_count)
    def _(i):
        tile = (2 * c + i) % tp_count
        total, normed = stream(pl.ds(pl.multiple_of(tile * share, share), share))
        rows[tile_at(y, tile), :] = normed

        @pl.when(tile == t)
        def _():
            resid[...] = total

        @pl.when(i < 2)
        def _():
            tile_copy(i, tile).start()

    wait_recv(block(1, z, 1 - y), wsend_sem.at[1, 0, 4], wrecv_sem.at[1, z, 1 - y])
    near_copies(1, 1)
    outer_far(1, 1)

    def pass_copy(i):
        ref = rows.at[tile_at(1 - y, 2 * c + i), :]
        return copy(ref, ref, tsend_sem.at[2 + i], trecv_sem.at[2 * c + i], z, y, t_core)

    towards = 1 + 2 * (z % 2)

    def source(step):
        return (z + step * towards) % 4

    def weights_here(m, step):
        zk = source(step)
        if step > 0:
            @pl.when(jnp.logical_not(inner & ((zk == far) | (zk == 3 - z))))
            def _():
                for h in range(2):
                    wait_recv(block(m, zk, h), wsend_sem.at[m, h, 3], wrecv_sem.at[m, zk, h])

    def project(m, step, first_row, size, tiles):
        zk = source(step)

        def tile(i):
            at = pl.ds(pl.multiple_of(first_row + i * size, EDGE), size)
            part = nt_dot(rows[at, cols(zk, wide)], wbuf[m, zk])
            if step == 0:
                acc[m, at, :] = part
            else:
                acc[m, at, :] += part

        if tiles == 1:
            tile(0)
        else:
            pl.loop(0, tiles)(tile)

    tall = tok_rows // 2

    def project_own(m, step):
        project(m, step, EDGE + y * tok_rows, tall, 2)

    def project_other(m, step):
        project(m, step, EDGE + (1 - y) * tok_rows, tall, 2)
        project(m, step, 0, EDGE, 1)

    for step in range(4):
        weights_here(0, step)
        project_own(0, step)
        if step == 1:
            for h in (y, 1 - y):
                pass_line(0, h, "far")
    pass_line(1, 1 - y, "near")
    for h in (y, 1 - y):
        pass_line(1, h, "far")
    wait_recv(block(2, z, 1 - y), wsend_sem.at[2, 0, 4], wrecv_sem.at[2, z, 1 - y])
    for h in range(2):
        near_copies(2, h)
        outer_far(2, h)
    for i in range(2):
        ref = rows.at[tile_at(1 - y, 2 * c + i), :]
        wait_recv(ref, tsend_sem.at[2 + i], trecv_sem.at[2 * c + i])
        pass_copy(i).start()
    for i in range(2):
        ref = rows.at[tile_at(1 - y, 2 * (1 - c) + i), :]
        wait_recv(ref, tsend_sem.at[2 + i], trecv_sem.at[2 * (1 - c) + i])

    @pl.when(z > 0)
    def _():
        wait_recv(head, tsend_sem.at[4], trecv_sem.at[tp_count])

    for step in range(4):
        project_other(0, step)
    for h in range(2):
        pass_line(2, h, "near")
    for step in range(4):
        weights_here(1, step)
        project_own(1, step)
        project_other(1, step)
        if step == 2:
            for h in range(2):
                pass_line(2, h, "far")

    @pl.loop(0, 2 * tok_rows // share)
    def _(i):
        at = pl.ds(pl.multiple_of(i * share, EDGE), share + EDGE)

        def mix(m):
            up = acc[m, at, :].astype(jnp.bfloat16).astype(jnp.float32)
            total = jnp.zeros_like(up)
            for j in range(CONV):
                back = CONV - 1 - j
                moved = up if back == 0 else pltpu.roll(up, back, 0)
                total = total + taps[m * CONV + j : m * CONV + j + 1, :] * moved
            return total[EDGE:, :]

        gate = mix(0)
        to = pl.ds(pl.multiple_of(i * share, share), share)
        hid[to, :] = (gate * jax.nn.sigmoid(gate) * mix(1)).astype(jnp.bfloat16)


    count = 8

    def down(b):
        zk, h = source(b // 2), b % 2
        if b >= 2:
            @pl.when(jnp.logical_not(inner & ((zk == far) | (zk == 3 - z))))
            def _():
                wait_recv(block(2, zk, h), wsend_sem.at[2, h, 3], wrecv_sem.at[2, zk, h])
        weight = wbuf[2, zk, :, h * depth : (h + 1) * depth]

        @pl.loop(0, tp_count)
        def _(j):
            give = pl.ds(pl.multiple_of((2 * j + 1 - c) * share, share), share)
            keep = pl.ds(pl.multiple_of((2 * j + c) * share, share), share)
            csend[b, j] = jnp.dot(hid[give, :], weight, preferred_element_type=jnp.float32).astype(jnp.bfloat16)
            ckeep[b % 2, j] = jnp.dot(hid[keep, :], weight, preferred_element_type=jnp.float32)

        c_copy(b).start()

    def c_copy(b):
        return copy(csend.at[b], crecv.at[b], csend_sem.at[b], crecv_sem.at[b], z, y, t_core)

    def second(b):
        to = (z, 1 - y, t) if b % 2 == 0 else (z, y, t_chip)
        return copy(ysend.at[b], yrecv.at[b], ysend_sem.at[b], yrecv_sem.at[b], *to)

    def third(b):
        to = (z, y, t_chip) if b % 2 == 0 else (z, 1 - y, t)
        return copy(xsend.at[b], xrecv.at[b], xsend_sem.at[b], xrecv_sem.at[b], *to)

    def over_c(b):
        c_copy(b).wait()
        even = b % 2 == 0
        for i in range(2):
            j = (1 - y) * 2 + i if even else i * 2 + 1 - x
            ysend[b, i] = (ckeep[b % 2, j] + crecv[b, j].astype(jnp.float32)).astype(jnp.bfloat16)
        second(b).start()
        for i in range(2):
            j = y * 2 + i if even else i * 2 + x
            ykeep[b % 2, i] = ckeep[b % 2, j] + crecv[b, j].astype(jnp.float32)

    def over_second(b):
        second(b).wait()
        keep = x if b % 2 == 0 else y
        xsend[b] = (ykeep[b % 2, 1 - keep] + yrecv[b, 1 - keep].astype(jnp.float32)).astype(jnp.bfloat16)
        third(b).start()
        xkeep[b % 2] = ykeep[b % 2, keep] + yrecv[b, keep].astype(jnp.float32)

    def over_third(b):
        third(b).wait()
        at = pl.ds(pl.multiple_of(source(b // 2) * wide + b % 2 * depth, depth), depth)
        total = resid[:, at] + (xkeep[b % 2] + xrecv[b].astype(jnp.float32))
        out[:, at] = total.astype(out.dtype)

    for b in range(count + 5):
        if 0 <= b - 5:
            over_third(b - 5)
        if 0 <= b - 3 < count:
            over_second(b - 3)
        if 0 <= b - 1 < count:
            over_c(b - 1)
        if b < count:
            down(b)

    def finish(one):
        one.wait_send()

    for m in range(3):
        finish(hop(m))
        for h in range(2):
            for one, cond in line_copies(m, h)[1:]:
                pl.when(cond)(functools.partial(finish, one))
            pl.when(jnp.logical_not(inner))(functools.partial(finish, line_copies(m, h)[0][0]))
            for origin in ("near", "far"):
                pl.when(inner)(functools.partial(finish, relay(m, h, origin)))
    for src, buf, send, recv in (
        (osrc, obuf, osend_sem, orecv_sem),
        (mixbuf.at[t], mixbuf, msend_sem, mrecv_sem),
    ):
        for one in tp_copies(src, buf, send, recv):
            finish(one)
        finish(tp_relay(buf, send, recv))
    finish(pair_copy())
    for d in range(1, pairs):
        pl.when(z + d < pairs)(functools.partial(finish, state_copy(d)))
    for i in range(2):
        finish(tile_copy(i, 2 * c + i))
        finish(pass_copy(i))

    @pl.when((y == 1) & (z < 3))
    def _():
        finish(edge_copy(0))
        finish(edge_copy(1))


def fused_layer(
    residual_input_stream,
    projected_queries,
    projected_keys,
    projected_values,
    emitted_switch_entries,
    retention_preactivations,
    additional_fading_amount,
    head_norm_gain,
    attention_output_weight,
    feedforward_norm_gain,
    gate_up_matrix,
    value_up_matrix,
    gate_filter_taps,
    value_filter_taps,
    down_projection_weight,
):
    tok_rows, width = residual_input_stream.shape
    keys, vals = projected_queries.shape[1], projected_values.shape[1]
    depth, units = gate_up_matrix.shape
    half, tp = units // 2, lax.axis_size("tp")
    share = tok_rows // tp
    bf16, f32, dma = jnp.bfloat16, jnp.float32, pltpu.SemaphoreType.DMA
    hbm, vmem = pl.BlockSpec(memory_space=pl.ANY), pl.BlockSpec(memory_space=pltpu.VMEM)
    scratch = [
        pltpu.VMEM((2, units, depth), bf16),
        pltpu.VMEM((8, half), f32),
        pltpu.VMEM((3, 4, half, 2 * depth), bf16),
        pltpu.VMEM((tp, vals, width), bf16),
        pltpu.VMEM((tp, tok_rows, vals), bf16),
        pltpu.VMEM((EDGE + 2 * tok_rows, width), bf16),
        pltpu.VMEM((2, EDGE + 2 * tok_rows, half), f32),
        pltpu.VMEM((2 * tok_rows, half), bf16),
        pltpu.VMEM((tok_rows, vals), f32),
        pltpu.VMEM((tok_rows, keys), f32),
        pltpu.VMEM((vals, keys), f32),
        pltpu.VMEM((8, keys), f32),
        pltpu.VMEM((DV + 8, keys), f32),
        pltpu.VMEM((DV + 8, keys), f32),
        pltpu.VMEM((EDGE, width), bf16),
        pltpu.VMEM((4, DV + 8, keys), f32),
        pltpu.VMEM((DV, keys), f32),
        pltpu.VMEM((share, width), f32),
        pltpu.VMEM((8, 4, share, depth), bf16),
        pltpu.VMEM((8, 4, share, depth), bf16),
        pltpu.VMEM((2, 4, share, depth), f32),
        pltpu.VMEM((8, 2, share, depth), bf16),
        pltpu.VMEM((8, 2, share, depth), bf16),
        pltpu.VMEM((2, 2, share, depth), f32),
        pltpu.VMEM((8, share, depth), bf16),
        pltpu.VMEM((8, share, depth), bf16),
        pltpu.VMEM((2, share, depth), f32),
        dma((3, 4, 2)), dma((3, 2, 5)), dma((tp,)), dma((3,)), dma((tp,)), dma((3,)), dma((4,)), dma((4,)),
        dma((tp + 1,)), dma((6,)), dma((8,)), dma((8,)), dma((8,)), dma((8,)), dma((8,)), dma((8,)),
    ]
    return pl.pallas_call(
        layer_kernel,
        name="layer",
        out_shape=jax.ShapeDtypeStruct((share, width), bf16),
        in_specs=[vmem] * 3 + [hbm] + [vmem] * 11,
        out_specs=vmem,
        scratch_shapes=scratch,
        compiler_params=pltpu.CompilerParams(
            collective_id=0, has_side_effects=True, vmem_limit_bytes=67043328
        ),
    )(
        gate_up_matrix, value_up_matrix, down_projection_weight, attention_output_weight, projected_queries, projected_keys, projected_values,
        emitted_switch_entries, retention_preactivations,
        additional_fading_amount.reshape(-1, BLOCK), residual_input_stream, head_norm_gain[None], feedforward_norm_gain[None],
        gate_filter_taps, value_filter_taps,
    )


def specs(rows):
    return (
            P(rows, None),
            P(rows, "tp"),
            P(rows, "tp"),
            P(rows, "tp"),
            P(rows, "tp"),
            P(rows, "tp"),
            P(rows),
            P(),
            P("tp", None),
            P(),
            P(rows, "tp"),
            P(rows, "tp"),
            P(None, "tp"),
            P(None, "tp"),
            P("tp", rows),
    )


def solution(mesh):
    sp, tp = mesh.shape["sp"], mesh.shape["tp"]
    if sp == 8 and tp == 4:
        return jax.shard_map(
            fused_layer,
            mesh=mesh,
            in_specs=specs("sp"),
            out_specs=P(("sp", "tp"), None),
            check_vma=False,
        )
    split = Mesh(mesh.devices.reshape(sp // 2, 2, tp), ("so", "si", "tp"))
    return jax.shard_map(
        per_device, mesh=split, in_specs=specs(SP), out_specs=P(("so", "si", "tp"), None), check_vma=False
    )
```

```python
import functools

import jax
import jax.numpy as jnp
from jax import lax
from jax.experimental import pallas as pl
from jax.experimental.pallas import tpu as pltpu
from jax.sharding import Mesh, PartitionSpec as P

DK = 64
DV = 128
CONV = 3
BLOCK = 64
EDGE = 16
SP = ("so", "si")


eps = 1e-06
retention_sharpness = 16.0


def from_behind(block, axis, distance):
    devices = range(lax.axis_size(axis))
    route = [(i - distance, i) for i in devices if i - distance in devices]
    return lax.ppermute(block, axis, route)


def to_blocks(tensor, local_heads, width):
    count = tensor.shape[0] // BLOCK
    return tensor.astype(jnp.float32).reshape(count, BLOCK, local_heads, width)


def row_norm(stream, gain):
    scaled = stream * lax.rsqrt(jnp.mean(stream * stream, axis=-1, keepdims=True) + eps)
    return (scaled * gain).astype(jnp.bfloat16)


def state_before_device(dev_log, dev_state):
    heads, channels, width = dev_state.shape
    lanes = heads * channels
    decay = jnp.pad(jnp.exp(dev_log).reshape(1, lanes), ((0, 0), (0, -lanes % width)))
    decay = decay.reshape(-1, width)
    packed = jnp.concatenate([dev_state.reshape(lanes, width), decay], axis=0)
    arriving = jnp.zeros_like(dev_state)
    after = jnp.ones((heads, channels), jnp.float32)
    for distance in range(1, lax.axis_size("so") * lax.axis_size("si")):
        got = from_behind(packed, SP, distance)
        arriving = arriving + after[..., None] * got[:lanes].reshape(dev_state.shape)
        after = after * got[lanes:].reshape(-1)[:lanes].reshape(after.shape)
    return arriving


def xor_route(axis, bit):
    return [(i, i ^ bit) for i in range(lax.axis_size(axis))]


def exchange(block, axis, bit):
    return lax.ppermute(block, axis, xor_route(axis, bit))


def gather_tp(block):
    count, me = lax.axis_size("tp"), lax.axis_index("tp")
    held = block[None]
    bit = count // 2
    while bit:
        other = exchange(held, "tp", bit)
        low = (me & bit) == 0
        held = jnp.stack([jnp.where(low, held, other), jnp.where(low, other, held)])
        held = held.reshape((-1,) + block.shape)
        bit //= 2
    bits = count.bit_length() - 1
    order = [sum(((t >> b) & 1) << (bits - 1 - b) for b in range(bits)) for t in range(count)]
    return [held[o] for o in order]


def swap_halves(block):
    first = lax.axis_index("si") == 0
    half = block.shape[0] // 2
    low, high = block[:half], block[half:]
    keep, give = jnp.where(first, low, high), jnp.where(first, high, low)
    got = exchange(give, "si", 1)
    return jnp.concatenate([jnp.where(first, keep, got), jnp.where(first, got, keep)], axis=1)


def line_gather(block):
    count, me = lax.axis_size("so"), lax.axis_index("so")
    if count != 4:
        whole = lax.all_gather(block, "so", axis=0)
        return [lax.dynamic_index_in_dim(whole, (me + k) % count, 0, False) for k in range(count)]
    across = lax.ppermute(block, "so", [(i, i ^ 2) for i in range(4)])
    above = lax.ppermute(block, "so", [(1, 0), (2, 1), (3, 2)])
    below = lax.ppermute(block, "so", [(0, 1), (1, 2), (2, 3)])
    far = lax.ppermute(across, "so", [(1, 0), (2, 3)])
    return [block, jnp.where(me == 3, far, above), across, jnp.where(me == 0, far, below)]


def pair_rows(normed):
    share = normed.shape[0] // 2
    mine = lax.axis_index("tp") % 2
    part = exchange(lax.dynamic_slice_in_dim(normed, mine * share, share, 0), "si", 1)
    other = exchange(part, "tp", 1)
    first = mine == 0
    return jnp.concatenate([jnp.where(first, part, other), jnp.where(first, other, part)], axis=0)


def project(rows, lines, width):
    count, me = lax.axis_size("so"), lax.axis_index("so")
    total = 0.0
    for k, line in enumerate(lines):
        part = lax.dynamic_slice_in_dim(rows, (me + k) % count * width, width, 1)
        total = total + lax.dot_general(
            part, line, (((1,), (1,)), ((), ())), preferred_element_type=jnp.float32
        )
    return total.astype(jnp.bfloat16)


def depthwise(before, body, taps):
    padded = jnp.concatenate([before, body], axis=0)
    start = padded.shape[0] - body.shape[0] - (CONV - 1)
    result = jnp.zeros(body.shape, jnp.float32)
    for offset in range(CONV):
        result = result + taps[offset].astype(jnp.float32)[None] * padded[
            start + offset : start + offset + body.shape[0]
        ].astype(jnp.float32)
    return result


def my_half(taps):
    half = taps.shape[1] // 2
    return jnp.where(lax.axis_index("si") == 0, taps[:, :half], taps[:, half:])


def halve(held, axis, bit):
    mine = (lax.axis_index(axis) // bit) % 2
    keep = lax.dynamic_index_in_dim(held, mine, 1, False)
    give = lax.dynamic_index_in_dim(held, 1 - mine, 1, False)
    got = exchange(give.astype(jnp.bfloat16), axis, bit)
    return keep.astype(jnp.float32) + got.astype(jnp.float32)


def scatter_sum(own, other):
    count = lax.axis_size("tp")
    share = own.shape[0] // count
    held = jnp.concatenate([own, other], axis=0)
    held = halve(held.reshape(count, 2, share, -1), "tp", 1)
    held = held.reshape(2, count // 2, share, -1)
    got = exchange(held[1].astype(jnp.bfloat16), "si", 1)
    held = held[0] + got.astype(jnp.float32)
    bit = 2
    while bit < count:
        held = halve(held.reshape((-1, 2) + held.shape[1:]), "tp", bit)
        bit *= 2
    return held[0]


def per_device(
    residual_input_stream,
    projected_queries,
    projected_keys,
    projected_values,
    emitted_switch_entries,
    retention_preactivations,
    additional_fading_amount,
    head_norm_gain,
    attention_output_weight,
    feedforward_norm_gain,
    gate_up_matrix,
    value_up_matrix,
    gate_filter_taps,
    value_filter_taps,
    down_projection_weight,
):
    largest_exponent = lax.Precision.HIGHEST
    tok_rows = residual_input_stream.shape[0]
    local_heads = projected_queries.shape[1] // DK
    gate_lines = line_gather(swap_halves(gate_up_matrix.T))
    value_lines = line_gather(swap_halves(value_up_matrix.T))
    down_lines = line_gather(swap_halves(down_projection_weight))
    out_full = jnp.concatenate(gather_tp(attention_output_weight), axis=0)
    retention_logarithm = (
        jax.nn.log_sigmoid(retention_preactivations.astype(jnp.float32)) / retention_sharpness
        + additional_fading_amount[:, None]
    )
    scaled_q = to_blocks(projected_queries, local_heads, DK) * DK ** (-0.5)
    key_heads = to_blocks(projected_keys, local_heads, DK)
    value_heads = to_blocks(projected_values, local_heads, DV)
    rate_cum = jnp.cumsum(to_blocks(retention_logarithm, local_heads, DK), axis=1)
    block_total = rate_cum[:, -1]
    before_block = jnp.cumsum(block_total, axis=0) - block_total
    q_decayed = scaled_q * jnp.exp(rate_cum)
    k_growth = key_heads * jnp.exp(-rate_cum)
    fading_through_finish = key_heads * jnp.exp(block_total[:, None] - rate_cum)
    lower = jnp.tril(jnp.ones((BLOCK, BLOCK), bool))
    scores = jnp.einsum("nihk,njhk->nhij", q_decayed, k_growth, precision=largest_exponent)
    scores = jnp.where(lower[None, None], scores, 0.0)
    within = jnp.einsum("nhij,njhv->nihv", scores, value_heads, precision=largest_exponent)
    increments = jnp.einsum(
        "nchk,nchv->nhkv", fading_through_finish, value_heads, precision=largest_exponent
    )

    count = block_total.shape[0]
    ends = before_block + block_total
    reached = jnp.concatenate([before_block, ends[-1:]], axis=0)
    earlier_block = jnp.arange(count)[None, :] < jnp.arange(count + 1)[:, None]
    fade = jnp.where(
        earlier_block[..., None, None],
        jnp.exp(jnp.minimum(reached[:, None] - ends[None], 0.0)),
        0.0,
    )
    states = jnp.sum(fade[..., None] * increments[None], axis=1)
    state_before, dev_state = states[:-1], states[-1]
    earlier = jnp.einsum("nchk,nhkv->nchv", q_decayed, state_before, precision=largest_exponent)
    query_shard = scaled_q * jnp.exp(rate_cum + before_block[:, None])
    dev_log = jnp.sum(block_total, axis=0)

    arriving_state = state_before_device(dev_log, dev_state)
    earlier_memory_share = jnp.einsum(
        "osyq,yqi->osyi", query_shard, arriving_state, precision=largest_exponent
    )
    mech_out = (within + earlier + earlier_memory_share).reshape(tok_rows, local_heads, DV)
    mech_out = (
        mech_out
        * lax.rsqrt(jnp.mean(mech_out * mech_out, axis=-1, keepdims=True) + eps)
        * head_norm_gain
    )
    mixed = (
        mech_out.reshape(tok_rows, local_heads * DV)
        * jax.nn.silu(emitted_switch_entries.astype(jnp.float32))
    ).astype(jnp.bfloat16)
    tp_count, tp_index = (lax.axis_size("tp"), lax.axis_index("tp"))
    share = tok_rows // tp_count
    mixed_all = jnp.concatenate(gather_tp(mixed), axis=1)
    attended = jnp.dot(mixed_all, out_full, preferred_element_type=jnp.float32)
    resid = residual_input_stream.astype(jnp.float32) + attended
    normed = row_norm(resid, feedforward_norm_gain)
    resid_own = lax.dynamic_slice_in_dim(resid, tp_index * share, share, 0)
    edge = normed[tok_rows - EDGE :]
    so_count, so_index = lax.axis_size("so"), lax.axis_index("so")
    first = lax.axis_index("si") == 0
    tail = jnp.where(first, from_behind(edge, SP, 1), from_behind(edge, "so", 1))
    width = 2 * gate_up_matrix.shape[0]
    other = pair_rows(normed)
    mine = jnp.concatenate([tail, normed], axis=0)
    gate_own = project(mine, gate_lines, width)
    value_own = project(mine, value_lines, width)
    gate_other = project(other, gate_lines, width)
    value_other = project(other, value_lines, width)

    def mix(up_own, up_other, taps):
        taps = my_half(taps)
        up_tail, up_own = up_own[:EDGE], up_own[EDGE:]
        own_end, other_end = up_own[tok_rows - EDGE :], up_other[tok_rows - EDGE :]
        own = depthwise(jnp.where(first, up_tail, other_end), up_own, taps)
        far = depthwise(jnp.where(first, own_end, up_tail), up_other, taps)
        return own, far

    gates = mix(gate_own, gate_other, gate_filter_taps)
    values = mix(value_own, value_other, value_filter_taps)
    hidden = [(jax.nn.silu(g) * v).astype(jnp.bfloat16) for g, v in zip(gates, values)]
    feed = jnp.zeros((share, resid.shape[1]), jnp.float32)
    for k, line in enumerate(down_lines):
        part = scatter_sum(*[jnp.dot(h, line, preferred_element_type=jnp.float32) for h in hidden])
        feed = lax.dynamic_update_slice_in_dim(feed, part, (so_index + k) % so_count * width, 1)
    return (resid_own + feed).astype(jnp.bfloat16)


def nt_dot(a, b, precision=None):
    return lax.dot_general(
        a, b, (((1,), (1,)), ((), ())), precision=precision, preferred_element_type=jnp.float32
    )


def layer_kernel(
    gate_in, value_in, down_in, osrc, q, k, v, gates, retention, fading, res, hgain, fgain, gate_taps, value_taps,
    out,
    wsrc, taps, wbuf, obuf, mixbuf, rows, acc, hid, mech, qs, state, before, packed, joined, edge, got, arrived, resid,
    csend, crecv, ckeep, ysend, yrecv, ykeep, xsend, xrecv, xkeep,
    wrecv_sem, wsend_sem, orecv_sem, osend_sem, mrecv_sem, msend_sem, srecv_sem, ssend_sem,
    trecv_sem, tsend_sem, crecv_sem, csend_sem, yrecv_sem, ysend_sem, xrecv_sem, xsend_sem,
):
    highest = lax.Precision.HIGHEST
    s, t = lax.axis_index("sp"), lax.axis_index("tp")
    z, y, x, c = s // 2, s % 2, t // 2, t % 2
    sp_count, tp_count = lax.axis_size("sp"), lax.axis_size("tp")
    tok_rows, (units, depth) = q.shape[0], down_in.shape
    half = units // 2
    share = out.shape[0]
    wide = 2 * depth

    def copy(src, dst, send, recv, zz, yy, tt):
        return pltpu.make_async_remote_copy(
            src_ref=src, dst_ref=dst, send_sem=send, recv_sem=recv,
            device_id=(zz * 2 + yy, tt), device_id_type=pl.DeviceIdType.MESH,
        )

    def wait_recv(ref, send, recv):
        copy(ref, ref, send, recv, z, y, t).wait_recv()

    def wait_send(ref, send, recv):
        copy(ref, ref, send, recv, z, y, t).wait_send()

    def cols(index, width):
        return pl.ds(pl.multiple_of(index * width, width), width)

    t_core, t_chip, t_diag = x * 2 + 1 - c, (1 - x) * 2 + c, (1 - x) * 2 + 1 - c

    wsrc[0] = jnp.transpose(gate_in[...])
    first = y == 0
    for m, given in enumerate((gate_taps, value_taps)):
        both = given[...].astype(jnp.float32)
        taps[m * CONV : (m + 1) * CONV, :] = jnp.where(first, both[:, :half], both[:, half:])

    barrier = pltpu.get_barrier_semaphore()

    @pl.loop(0, sp_count * tp_count)
    def _(i):
        pl.semaphore_signal(
            barrier, inc=1, device_id=(i // tp_count, i % tp_count), device_id_type=pl.DeviceIdType.MESH
        )

    pl.semaphore_wait(barrier, sp_count * tp_count)

    def block(m, zz, h):
        return wbuf.at[m, zz, :, cols(h, depth)]

    def half_of(m, h):
        at = pl.ds(pl.multiple_of(h * half, half), half)
        return down_in.at[at, :] if m == 2 else wsrc.at[m, at, :]

    def place_own(m):
        wbuf[m, z, :, cols(y, depth)] = half_of(m, y)[...]

    def hop(m):
        return copy(half_of(m, 1 - y), block(m, z, y), wsend_sem.at[m, 0, 4], wrecv_sem.at[m, z, y], z, 1 - y, t)

    far = (z + 2) % 4

    def line_copies(m, slot):
        h = slot if m == 2 else (y if slot == 0 else 1 - y)
        src = half_of(m, y) if m < 2 and slot == 0 else block(m, z, h)
        dests = ((far, None), (z + 1, z < 3), (z - 1, z > 0))
        return [
            (copy(src, block(m, z, h), wsend_sem.at[m, slot, i], wrecv_sem.at[m, z, h], dest, y, t), cond)
            for i, (dest, cond) in enumerate(dests)
        ]

    def each(copies, act):
        for one, cond in copies:
            if cond is None:
                act(one)
            else:
                pl.when(cond)(functools.partial(act, one))

    def start(one):
        one.start()

    inner = (z > 0) & (z < 3)

    def near_copies(m, slot):
        each(line_copies(m, slot)[1:], start)

    def outer_far(m, slot):
        pl.when(jnp.logical_not(inner))(functools.partial(start, line_copies(m, slot)[0][0]))

    def far_of(end, m):
        @pl.when(z == end)
        def _():
            for slot in range(2):
                line_copies(m, slot)[0][0].start()

    def relay(m, h, origin):
        zz, index = (far, 3) if origin == "far" else (3 - z, 0)
        return copy(
            block(m, zz, h), block(m, zz, h), wsend_sem.at[m, h, index], wrecv_sem.at[m, zz, h], 3 * (z - 1), y, t
        )

    def pass_line(m, h, origin):
        @pl.when(inner)
        def _():
            zz, index = (far, 3) if origin == "far" else (3 - z, 0)
            wait_recv(block(m, zz, h), wsend_sem.at[m, h, index], wrecv_sem.at[m, zz, h])
            relay(m, h, origin).start()

    def tp_copies(src, buf, send, recv):
        return (
            copy(src, buf.at[t], send.at[0], recv.at[t], z, y, t_core),
            copy(src, buf.at[t], send.at[1], recv.at[t], z, y, t_chip),
        )

    def tp_relay(buf, send, recv):
        return copy(buf.at[t_chip], buf.at[t_chip], send.at[2], recv.at[t_chip], z, y, t_core)

    def tp_pass_on(buf, send, recv):
        wait_recv(buf.at[t_chip], send.at[2], recv.at[t_chip])
        tp_relay(buf, send, recv).start()

    def tp_arrive(buf, send, recv):
        wait_recv(buf.at[t_core], send.at[0], recv.at[t_core])
        wait_recv(buf.at[t_diag], send.at[0], recv.at[t_diag])

    hop(0).start()
    near_copies(0, 0)
    own_out = pltpu.make_async_copy(osrc, obuf.at[t], orecv_sem.at[t])
    own_out.start()
    for one in tp_copies(osrc, obuf, osend_sem, orecv_sem):
        one.start()
    wsrc[1] = jnp.transpose(value_in[...])
    hop(1).start()
    for m in range(3):
        place_own(m)

    scale = DK ** (-0.5)
    key_lanes = q.shape[1]
    val_lanes = v.shape[1]
    lane_head = lax.broadcasted_iota(jnp.int32, (BLOCK, key_lanes), 1) // DK
    heads = key_lanes // DK
    low = lax.broadcasted_iota(jnp.int32, (BLOCK, BLOCK), 0) >= lax.broadcasted_iota(jnp.int32, (BLOCK, BLOCK), 1)
    low_ones = low.astype(jnp.float32)
    fade_lanes = fading.shape[1]
    per_row = fade_lanes // BLOCK
    fade_lane = lax.broadcasted_iota(jnp.int32, (BLOCK, fade_lanes), 1)
    lane_block = fade_lane // BLOCK
    low_lanes = lax.broadcasted_iota(jnp.int32, (BLOCK, fade_lanes), 0) >= fade_lane % BLOCK
    same_head = (
        lax.broadcasted_iota(jnp.int32, (val_lanes, key_lanes), 0) // DV
        == lax.broadcasted_iota(jnp.int32, (val_lanes, key_lanes), 1) // DK
    )
    state[...] = jnp.zeros_like(state)
    before[...] = jnp.zeros_like(before)

    def attend_block(i):
        at = pl.ds(pl.multiple_of(i * BLOCK, BLOCK), BLOCK)
        gate = retention[at, :].astype(jnp.float32)
        rate = (jnp.minimum(gate, 0.0) - jnp.log1p(jnp.exp(-jnp.abs(gate)))) / retention_sharpness
        behind = low_lanes & (lane_block == i % per_row)
        faded = jnp.sum(jnp.where(behind, fading[pl.ds(i // per_row, 1), :], 0.0), axis=1, keepdims=True)
        cum = jnp.dot(low_ones, rate, precision=highest, preferred_element_type=jnp.float32) + faded
        total = cum[BLOCK - 1 :, :]
        ahead = before[0:1, :]
        q_decayed = q[at, :].astype(jnp.float32) * scale * jnp.exp(cum)
        qs[at, :] = q[at, :].astype(jnp.float32) * scale * jnp.exp(cum + ahead)
        keys = k[at, :].astype(jnp.float32)
        grown = keys * jnp.exp(-cum)
        ending = keys * jnp.exp(total - cum)
        values = v[at, :].astype(jnp.float32)
        inside = []
        for h in range(heads):
            mine = lane_head == h
            scores = nt_dot(jnp.where(mine, q_decayed, 0.0), jnp.where(mine, grown, 0.0), highest)
            scores = jnp.where(low, scores, 0.0)
            inside.append(
                jnp.dot(
                    scores, values[:, h * DV : (h + 1) * DV], precision=highest, preferred_element_type=jnp.float32
                )
            )
        old = state[...]
        mech[at, :] = jnp.concatenate(inside, axis=1) + nt_dot(q_decayed, old, highest)
        step = lax.dot_general(
            values, ending, (((0,), (0,)), ((), ())), precision=highest, preferred_element_type=jnp.float32
        )
        state[...] = old * jnp.exp(total) + jnp.where(same_head, step, 0.0)
        before[...] = jnp.broadcast_to(ahead + total, before.shape)

    blocks = tok_rows // BLOCK
    early_blocks = 2 * blocks // 3
    pl.loop(0, early_blocks)(attend_block)
    wait_recv(block(0, z, 1 - y), wsend_sem.at[0, 0, 4], wrecv_sem.at[0, z, 1 - y])
    near_copies(0, 1)
    pass_line(0, y, "near")
    pl.loop(early_blocks, blocks)(attend_block)

    whole = state[0:DV, :]
    for h in range(1, heads):
        whole = whole + state[h * DV : (h + 1) * DV, :]
    packed[0:DV, :] = whole
    packed[DV:, :] = jnp.exp(before[...])
    pairs = sp_count // 2

    def pair_copy():
        return copy(packed, got.at[0], ssend_sem.at[0], srecv_sem.at[0], z, 1 - y, t)

    def state_copy(d):
        return copy(joined, got.at[d], ssend_sem.at[d], srecv_sem.at[d], z + d, y, t)

    pair_copy().start()
    hop(2).start()
    wait_recv(got.at[0], ssend_sem.at[0], srecv_sem.at[0])
    early = jnp.where(first, packed[...], got[0])
    late = jnp.where(first, got[0], packed[...])
    joined[0:DV, :] = early[0:DV, :] * late[DV : DV + 1, :] + late[0:DV, :]
    joined[DV:, :] = early[DV:, :] * late[DV:, :]
    for d in range(1, pairs):
        pl.when(z + d < pairs)(functools.partial(start, state_copy(d)))
    pass_line(0, 1 - y, "near")
    near_copies(1, 0)
    arrived[...] = jnp.zeros_like(arrived)
    before[...] = jnp.ones_like(before)
    for d in range(1, pairs):
        @pl.when(z >= d)
        def _(d=d):
            wait_recv(got.at[d], ssend_sem.at[d], srecv_sem.at[d])
            arrived[...] += before[0:1, :] * got[d, 0:DV, :]
            before[...] = before[...] * got[d, DV:, :]

    @pl.when(y == 1)
    def _():
        arrived[...] = arrived[...] * got[0, DV : DV + 1, :] + got[0, 0:DV, :]

    lane_wide = lax.broadcasted_iota(jnp.int32, (share, key_lanes), 1) // DK
    lane_state = lax.broadcasted_iota(jnp.int32, (DV, key_lanes), 1) // DK

    @pl.loop(0, tok_rows // share)
    def _(i):
        at = pl.ds(pl.multiple_of(i * share, share), share)
        for h in range(heads):
            part = pl.ds(h * DV, DV)
            extra = nt_dot(
                jnp.where(lane_wide == h, qs[at, :], 0.0), jnp.where(lane_state == h, arrived[...], 0.0), highest
            )
            o = mech[at, part] + extra
            o = o * lax.rsqrt(jnp.mean(o * o, axis=-1, keepdims=True) + eps) * hgain[...]
            gate = gates[at, part].astype(jnp.float32)
            mixbuf[t, at, part] = (o * (gate * jax.nn.sigmoid(gate))).astype(jnp.bfloat16)

    for one in tp_copies(mixbuf.at[t], mixbuf, msend_sem, mrecv_sem):
        one.start()
    far_of(3, 0)
    tp_pass_on(obuf, osend_sem, orecv_sem)
    tp_pass_on(mixbuf, msend_sem, mrecv_sem)
    own_out.wait()
    tp_arrive(obuf, osend_sem, orecv_sem)
    tp_arrive(mixbuf, msend_sem, mrecv_sem)

    def tile_at(yy, tile):
        return pl.ds(pl.multiple_of(EDGE + yy * tok_rows + tile * share, EDGE), share)

    def tile_copy(i, tile):
        ref = rows.at[tile_at(y, tile), :]
        return copy(ref, ref, tsend_sem.at[i], trecv_sem.at[tile], z, 1 - y, t)

    def stream(at):
        total = res[at, :].astype(jnp.float32)
        for part in range(tp_count):
            total = total + jnp.dot(mixbuf[part, at, :], obuf[part], preferred_element_type=jnp.float32)
        scaled = total * lax.rsqrt(jnp.mean(total * total, axis=-1, keepdims=True) + eps)
        return total, (scaled * fgain[...]).astype(jnp.bfloat16)

    head = rows.at[pl.ds(0, EDGE), :]

    def edge_copy(yy):
        return copy(edge, head, tsend_sem.at[4 + yy], trecv_sem.at[tp_count], z + 1, yy, t)

    @pl.when((y == 1) & (z < 3))
    def _():
        edge[...] = stream(pl.ds(tok_rows - EDGE, EDGE))[1]
        edge_copy(0).start()
        edge_copy(1).start()

    @pl.when(z == 0)
    def _():
        rows[0:EDGE, :] = jnp.zeros((EDGE, rows.shape[1]), rows.dtype)

    pass_line(1, y, "near")
    far_of(0, 0)

    @pl.loop(0, tp_count)
    def _(i):
        tile = (2 * c + i) % tp_count
        total, normed = stream(pl.ds(pl.multiple_of(tile * share, share), share))
        rows[tile_at(y, tile), :] = normed

        @pl.when(tile == t)
        def _():
            resid[...] = total

        @pl.when(i < 2)
        def _():
            tile_copy(i, tile).start()

    wait_recv(block(1, z, 1 - y), wsend_sem.at[1, 0, 4], wrecv_sem.at[1, z, 1 - y])
    near_copies(1, 1)
    far_of(0, 1)
    far_of(3, 1)

    def pass_copy(i):
        ref = rows.at[tile_at(1 - y, 2 * c + i), :]
        return copy(ref, ref, tsend_sem.at[2 + i], trecv_sem.at[2 * c + i], z, y, t_core)

    towards = 1 + 2 * (z % 2)

    def source(step):
        return (z + step * towards) % 4

    def weights_here(m, step):
        zk = source(step)
        if step > 0:
            @pl.when(jnp.logical_not(inner & ((zk == far) | (zk == 3 - z))))
            def _():
                for h in range(2):
                    wait_recv(block(m, zk, h), wsend_sem.at[m, h, 3], wrecv_sem.at[m, zk, h])

    def project(m, step, first_row, size, tiles):
        zk = source(step)

        def tile(i):
            at = pl.ds(pl.multiple_of(first_row + i * size, EDGE), size)
            part = nt_dot(rows[at, cols(zk, wide)], wbuf[m, zk])
            if step == 0:
                acc[m, at, :] = part
            else:
                acc[m, at, :] += part

        if tiles == 1:
            tile(0)
        else:
            pl.loop(0, tiles)(tile)

    tall = tok_rows // 2

    def project_own(m, step):
        project(m, step, EDGE + y * tok_rows, tall, 2)

    def project_other(m, step):
        project(m, step, EDGE + (1 - y) * tok_rows, tall, 2)
        project(m, step, 0, EDGE, 1)

    for step in range(4):
        weights_here(0, step)
        project_own(0, step)
        if step == 1:
            for h in (y, 1 - y):
                pass_line(0, h, "far")
    pass_line(1, 1 - y, "near")
    for h in (y, 1 - y):
        pass_line(1, h, "far")
    wait_recv(block(2, z, 1 - y), wsend_sem.at[2, 0, 4], wrecv_sem.at[2, z, 1 - y])
    for h in range(2):
        near_copies(2, h)
        outer_far(2, h)
    for i in range(2):
        ref = rows.at[tile_at(1 - y, 2 * c + i), :]
        wait_recv(ref, tsend_sem.at[2 + i], trecv_sem.at[2 * c + i])
        pass_copy(i).start()
    for i in range(2):
        ref = rows.at[tile_at(1 - y, 2 * (1 - c) + i), :]
        wait_recv(ref, tsend_sem.at[2 + i], trecv_sem.at[2 * (1 - c) + i])

    @pl.when(z > 0)
    def _():
        wait_recv(head, tsend_sem.at[4], trecv_sem.at[tp_count])

    for step in range(4):
        project_other(0, step)
    for step in range(4):
        weights_here(1, step)
        project_own(1, step)
        project_other(1, step)

    for h in range(2):
        pass_line(2, h, "near")

    @pl.loop(0, 2 * tok_rows // share)
    def _(i):
        at = pl.ds(pl.multiple_of(i * share, EDGE), share + EDGE)

        def mix(m):
            up = acc[m, at, :].astype(jnp.bfloat16).astype(jnp.float32)
            total = jnp.zeros_like(up)
            for j in range(CONV):
                back = CONV - 1 - j
                moved = up if back == 0 else pltpu.roll(up, back, 0)
                total = total + taps[m * CONV + j : m * CONV + j + 1, :] * moved
            return total[EDGE:, :]

        gate = mix(0)
        to = pl.ds(pl.multiple_of(i * share, share), share)
        hid[to, :] = (gate * jax.nn.sigmoid(gate) * mix(1)).astype(jnp.bfloat16)


    for h in range(2):
        pass_line(2, h, "far")

    count = 8

    def down(b):
        zk, h = source(b // 2), b % 2
        if b >= 2:
            @pl.when(jnp.logical_not(inner & ((zk == far) | (zk == 3 - z))))
            def _():
                wait_recv(block(2, zk, h), wsend_sem.at[2, h, 3], wrecv_sem.at[2, zk, h])
        weight = wbuf[2, zk, :, h * depth : (h + 1) * depth]

        @pl.loop(0, tp_count)
        def _(j):
            give = pl.ds(pl.multiple_of((2 * j + 1 - c) * share, share), share)
            keep = pl.ds(pl.multiple_of((2 * j + c) * share, share), share)
            csend[b, j] = jnp.dot(hid[give, :], weight, preferred_element_type=jnp.float32).astype(jnp.bfloat16)
            ckeep[b % 2, j] = jnp.dot(hid[keep, :], weight, preferred_element_type=jnp.float32)

        c_copy(b).start()

    def c_copy(b):
        return copy(csend.at[b], crecv.at[b], csend_sem.at[b], crecv_sem.at[b], z, y, t_core)

    def second(b, i):
        to = (z, 1 - y, t) if b % 2 == 0 else (z, y, t_chip)
        return copy(ysend.at[b, i], yrecv.at[b, i], ysend_sem.at[b, i], yrecv_sem.at[b, i], *to)

    def third(b):
        to = (z, y, t_chip) if b % 2 == 0 else (z, 1 - y, t)
        return copy(xsend.at[b], xrecv.at[b], xsend_sem.at[b], xrecv_sem.at[b], *to)

    def over_c(b):
        c_copy(b).wait()
        even = b % 2 == 0
        keep = x if even else y
        for i in (1 - keep, keep):
            j = (1 - y) * 2 + i if even else i * 2 + 1 - x
            ysend[b, i] = (ckeep[b % 2, j] + crecv[b, j].astype(jnp.float32)).astype(jnp.bfloat16)
            second(b, i).start()
        for i in range(2):
            j = y * 2 + i if even else i * 2 + x
            ykeep[b % 2, i] = ckeep[b % 2, j] + crecv[b, j].astype(jnp.float32)

    def over_second(b):
        keep = x if b % 2 == 0 else y
        second(b, 1 - keep).wait()
        xsend[b] = (ykeep[b % 2, 1 - keep] + yrecv[b, 1 - keep].astype(jnp.float32)).astype(jnp.bfloat16)
        third(b).start()
        second(b, keep).wait()
        xkeep[b % 2] = ykeep[b % 2, keep] + yrecv[b, keep].astype(jnp.float32)

    def over_third(b):
        third(b).wait()
        at = pl.ds(pl.multiple_of(source(b // 2) * wide + b % 2 * depth, depth), depth)
        total = resid[:, at] + (xkeep[b % 2] + xrecv[b].astype(jnp.float32))
        out[:, at] = total.astype(out.dtype)

    for b in range(count + 5):
        if 0 <= b - 5:
            over_third(b - 5)
        if 0 <= b - 3 < count:
            over_second(b - 3)
        if 0 <= b - 1 < count:
            over_c(b - 1)
        if b < count:
            down(b)

    def finish(one):
        one.wait_send()

    for m in range(3):
        finish(hop(m))
        for h in range(2):
            for one, cond in line_copies(m, h)[1:]:
                pl.when(cond)(functools.partial(finish, one))
            pl.when(jnp.logical_not(inner))(functools.partial(finish, line_copies(m, h)[0][0]))
            for origin in ("near", "far"):
                pl.when(inner)(functools.partial(finish, relay(m, h, origin)))
    for src, buf, send, recv in (
        (osrc, obuf, osend_sem, orecv_sem),
        (mixbuf.at[t], mixbuf, msend_sem, mrecv_sem),
    ):
        for one in tp_copies(src, buf, send, recv):
            finish(one)
        finish(tp_relay(buf, send, recv))
    finish(pair_copy())
    for d in range(1, pairs):
        pl.when(z + d < pairs)(functools.partial(finish, state_copy(d)))
    for i in range(2):
        finish(tile_copy(i, 2 * c + i))
        finish(pass_copy(i))

    @pl.when((y == 1) & (z < 3))
    def _():
        finish(edge_copy(0))
        finish(edge_copy(1))


def fused_layer(
    residual_input_stream,
    projected_queries,
    projected_keys,
    projected_values,
    emitted_switch_entries,
    retention_preactivations,
    additional_fading_amount,
    head_norm_gain,
    attention_output_weight,
    feedforward_norm_gain,
    gate_up_matrix,
    value_up_matrix,
    gate_filter_taps,
    value_filter_taps,
    down_projection_weight,
):
    tok_rows, width = residual_input_stream.shape
    keys, vals = projected_queries.shape[1], projected_values.shape[1]
    depth, units = gate_up_matrix.shape
    half, tp = units // 2, lax.axis_size("tp")
    share = tok_rows // tp
    bf16, f32, dma = jnp.bfloat16, jnp.float32, pltpu.SemaphoreType.DMA
    hbm, vmem = pl.BlockSpec(memory_space=pl.ANY), pl.BlockSpec(memory_space=pltpu.VMEM)
    scratch = [
        pltpu.VMEM((2, units, depth), bf16),
        pltpu.VMEM((8, half), f32),
        pltpu.VMEM((3, 4, half, 2 * depth), bf16),
        pltpu.VMEM((tp, vals, width), bf16),
        pltpu.VMEM((tp, tok_rows, vals), bf16),
        pltpu.VMEM((EDGE + 2 * tok_rows, width), bf16),
        pltpu.VMEM((2, EDGE + 2 * tok_rows, half), f32),
        pltpu.VMEM((2 * tok_rows, half), bf16),
        pltpu.VMEM((tok_rows, vals), f32),
        pltpu.VMEM((tok_rows, keys), f32),
        pltpu.VMEM((vals, keys), f32),
        pltpu.VMEM((8, keys), f32),
        pltpu.VMEM((DV + 8, keys), f32),
        pltpu.VMEM((DV + 8, keys), f32),
        pltpu.VMEM((EDGE, width), bf16),
        pltpu.VMEM((4, DV + 8, keys), f32),
        pltpu.VMEM((DV, keys), f32),
        pltpu.VMEM((share, width), f32),
        pltpu.VMEM((8, 4, share, depth), bf16),
        pltpu.VMEM((8, 4, share, depth), bf16),
        pltpu.VMEM((2, 4, share, depth), f32),
        pltpu.VMEM((8, 2, share, depth), bf16),
        pltpu.VMEM((8, 2, share, depth), bf16),
        pltpu.VMEM((2, 2, share, depth), f32),
        pltpu.VMEM((8, share, depth), bf16),
        pltpu.VMEM((8, share, depth), bf16),
        pltpu.VMEM((2, share, depth), f32),
        dma((3, 4, 2)), dma((3, 2, 5)), dma((tp,)), dma((3,)), dma((tp,)), dma((3,)), dma((4,)), dma((4,)),
        dma((tp + 1,)), dma((6,)), dma((8,)), dma((8,)), dma((8, 2)), dma((8, 2)), dma((8,)), dma((8,)),
    ]
    return pl.pallas_call(
        layer_kernel,
        name="layer",
        out_shape=jax.ShapeDtypeStruct((share, width), bf16),
        in_specs=[vmem] * 3 + [hbm] + [vmem] * 11,
        out_specs=vmem,
        scratch_shapes=scratch,
        compiler_params=pltpu.CompilerParams(
            collective_id=0, has_side_effects=True, vmem_limit_bytes=67043328
        ),
    )(
        gate_up_matrix, value_up_matrix, down_projection_weight, attention_output_weight, projected_queries, projected_keys, projected_values,
        emitted_switch_entries, retention_preactivations,
        additional_fading_amount.reshape(-1, 2 * BLOCK), residual_input_stream, head_norm_gain[None], feedforward_norm_gain[None],
        gate_filter_taps, value_filter_taps,
    )


def specs(rows):
    return (
            P(rows, None),
            P(rows, "tp"),
            P(rows, "tp"),
            P(rows, "tp"),
            P(rows, "tp"),
            P(rows, "tp"),
            P(rows),
            P(),
            P("tp", None),
            P(),
            P(rows, "tp"),
            P(rows, "tp"),
            P(None, "tp"),
            P(None, "tp"),
            P("tp", rows),
    )


def solution(mesh):
    sp, tp = mesh.shape["sp"], mesh.shape["tp"]
    if sp == 8 and tp == 4:
        return jax.shard_map(
            fused_layer,
            mesh=mesh,
            in_specs=specs("sp"),
            out_specs=P(("sp", "tp"), None),
            check_vma=False,
        )
    split = Mesh(mesh.devices.reshape(sp // 2, 2, tp), ("so", "si", "tp"))
    return jax.shard_map(
        per_device, mesh=split, in_specs=specs(SP), out_specs=P(("so", "si", "tp"), None), check_vma=False
    )
```
